128 devices in a mesh: ep: 32 (over z, y, core), tp: 4 (over x).
Axes of the slice: x: 4, y: 4, z: 4, core: 2. Of those that a mesh axis runs over, the one named last changes fastest.
Arguments:
- query_rows: bfloat16 [65536, 1024], P('ep', 'tp'), may hold values from -6 to 6
- key_rows: bfloat16 [65536, 1024], P('ep', 'tp'), may hold values from -6 to 6
- value_rows: bfloat16 [65536, 2048], P('ep', 'tp'), may hold values from -6 to 6
- gate_rows: bfloat16 [65536, 2048], P('ep', 'tp'), may hold values from -6 to 6
- log_decay: float32 [8, 65536], P('tp', 'ep'), may hold values from -1 to 0
- out_proj: bfloat16 [2048, 2048], P('tp'), may hold values from -0.125 to 0.125
- moe_input: bfloat16 [16384, 2048], P(('ep', 'tp')), may hold values from -6 to 6
- norm_gain: float32 [2048], replicated, may hold values from 0.1 to 1.9
- routing: int32 [16384, 4], P(('ep', 'tp')), may hold values from 0 to 127, all different within a row; in each aligned block of 128 rows (0 to 127, 128 to 255, ...) at most 8 rows name the same one
- route_weight: float32 [16384, 4], P(('ep', 'tp')), may hold values from 0.2 to 1
- expert_gate: bfloat16 [128, 2048, 512], P(('ep', 'tp')), may hold values from -0.125 to 0.125
- expert_up: bfloat16 [128, 2048, 512], P(('ep', 'tp')), may hold values from -0.125 to 0.125
- expert_down: bfloat16 [128, 512, 2048], P(('ep', 'tp')), may hold values from -0.25 to 0.25
- shared_gate: bfloat16 [2048, 512], replicated, may hold values from -0.125 to 0.125
- shared_up: bfloat16 [2048, 512], replicated, may hold values from -0.125 to 0.125
- shared_down: bfloat16 [512, 2048], replicated, may hold values from -0.25 to 0.25
Outputs:
- mixer_out: bfloat16 [65536, 2048], P(('ep', 'tp'))
- moe_out: bfloat16 [16384, 2048], P(('ep', 'tp'))
The draws below stay inside these ranges and needn't reach their ends.
Inputs may be any that keep to these rules, and one draw needn't show every extreme that they name: `routing`: within the rows of one device no expert is named more than 8 times.
All inputs are finite; a program needn't handle non-finite values.
Results may differ from the reference program's by a relative error of at most 0.019.
Values may be sent and summed in bfloat16 or wider, within the bound.
No kernel may reach another device: no remote copies, remote signals or barrier semaphores. Data moves between devices by JAX's collectives and lax.ppermute only.
A program may use at most 128 MiB of HBM per device.

```python
import math
import jax
import jax.numpy as jnp
import numpy as np
from jax import lax

D = 2048
RETENTION_HEADS = 8
DK = 128
DV = 256
BLOCK = 128
TOK_A = 2048
TOKENS_A = 65536
FF = 512
SHARED_FF = 512
TOP = 4
TOK_B = 128
TOKENS_B = 16384
EXPERTS = 128
CAP = 8
N_EP = 32
N_TP = 4


def draw_log_decay(key, part):
    random_subkeys = jax.random.split(jax.random.fold_in(key, 17), 7)
    sequence_length = TOKENS_A
    fast_share = 0.5
    quick_decay_mask = jax.random.uniform(random_subkeys[0], (RETENTION_HEADS,)) < fast_share
    fast_rate = jnp.log(10.0) / jax.random.uniform(random_subkeys[1], (RETENTION_HEADS,), minval=30.0, maxval=100.0)
    slow_rate = jax.random.uniform(random_subkeys[2], (RETENTION_HEADS,), minval=0.2, maxval=0.6) / sequence_length
    base_rate = jnp.where(quick_decay_mask, fast_rate, slow_rate)
    position_index = jnp.arange(sequence_length)
    span_factor = jnp.exp(jax.random.uniform(random_subkeys[3], (sequence_length // TOK_A,), minval=-0.7, maxval=0.7))
    jitter = jnp.exp(jax.random.uniform(random_subkeys[4], (RETENTION_HEADS, sequence_length), minval=-0.35, maxval=0.35))
    chosen_places = jax.random.randint(random_subkeys[5], (3,), 0, sequence_length)
    spike_selected = jnp.any(position_index[None, :] == chosen_places[:, None], axis=0)
    spike_dropped = jnp.log(jax.random.uniform(random_subkeys[6], (RETENTION_HEADS, sequence_length), minval=0.5, maxval=0.8))
    smoothed_decay = -base_rate[:, None] * span_factor[position_index // TOK_A][None, :] * jitter
    selected_mask = spike_selected[None, :] & jnp.logical_not(quick_decay_mask)[:, None]
    return jnp.where(selected_mask, smoothed_decay + spike_dropped, smoothed_decay).astype(jnp.float32)


def steps_of(rng, shape, cuts, smallest, top_value):
    def one(dim, shards_of):
        steps = jax.random.uniform(jax.random.fold_in(jax.random.fold_in(rng, 6), dim), (shards_of,), jnp.float32, smallest / len(cuts), top_value / len(cuts))
        return jnp.repeat(jnp.exp(steps), shape[dim] // shards_of).reshape((-1,) + (1,) * (len(shape) - dim - 1))

    loudness = one(*cuts[0])
    for cut in cuts[1:]:
        loudness = loudness * one(*cut)
    return loudness


def deal_out(rng, own, number, rows, count, top, limit, skew):
    sequence = jax.random.permutation(rng, count)
    crowded, common = portions_of(count, rows * top, limit, skew, True), portions_of(count, rows * top, limit, skew, False)
    places = jnp.arange(count)

    def named(tallies, rotation):
        used = int((tallies > 0).sum())
        fixed = max(1, used // 4)
        passed = fixed + (places - fixed + rotation * (used - fixed)) % max(1, count - fixed)
        return jnp.zeros((count,), jnp.int32).at[sequence[jnp.where(places < fixed, places, passed)]].set(jnp.asarray(tallies, jnp.int32))

    tallies = jnp.where(number % 4 == 0, named(crowded, number // 4), named(common, number - number // 4 - 1))
    mixed = jax.random.permutation(jax.random.fold_in(own, 3), count)
    giver, taker = mixed[0:count // 2 * 2:2], mixed[1:count // 2 * 2:2]
    margin = jnp.minimum(tallies[giver] - 1, limit - tallies[taker]) // 2
    margin = jnp.where((giver == sequence[0]) | (taker == sequence[0]) | (tallies[taker] == 0), 0, jnp.maximum(margin, 0))
    passed = jax.random.randint(jax.random.fold_in(own, 4), (count // 2,), 0, 1 << 20) % (margin + 1)
    tallies = tallies.at[giver].add(-passed).at[taker].add(passed)
    items = jnp.searchsorted(jnp.cumsum(tallies), jnp.arange(rows * top), side="right").astype(jnp.int32)
    listing = items.reshape(top, rows).T
    listing = listing[jax.random.permutation(jax.random.fold_in(own, 1), rows)]
    rotation = jax.random.randint(jax.random.fold_in(own, 2), (rows, 1), 0, top)
    return jnp.take_along_axis(listing, (jnp.arange(top)[None, :] + rotation) % top, axis=1)


def portions_of(number_of, total, most, skew, full):
    portions = [(1 << 20) // math.isqrt(rank ** skew) + 1 for rank in range(1, number_of + 1)]
    largest = most if full else min(most, max(-(-total // number_of), total * portions[0] // sum(portions)))
    least = 1 if total - largest >= number_of - 1 else 0
    given, spare = [largest] + [least] * (number_of - 1), total - largest - least * (number_of - 1)
    while spare > 0:
        candidates = [i for i in range(1, number_of) if given[i] < largest] or [i for i in range(1, number_of) if given[i] < most]
        whole, budget = sum([portions[i] for i in candidates]), spare
        for i in candidates:
            more = min(most - given[i], max(1, budget * portions[i] // whole), spare)
            given[i] = given[i] + more
            spare = spare - more
    return np.array(given)


def bell_draw(rng, shape, width, reach, pieces=(), held_as=jnp.bfloat16):
    loudness = steps_of(rng, shape, pieces, -0.22, 0.18) if pieces else 1.0
    entries = jax.random.normal(rng, shape, jnp.float32) * width * loudness
    return jnp.minimum(jnp.maximum(entries, -reach), reach).astype(held_as)


def setup_inputs(seed: int = 0) -> dict:
    keys = jax.random.split(jax.random.key(seed), 17)
    query_rows = bell_draw(keys[0], (TOKENS_A, RETENTION_HEADS * DK), 1.0, 6.0, ((0, 32), (1, 4)))
    key_rows = bell_draw(keys[1], (TOKENS_A, RETENTION_HEADS * DK), 1.0, 6.0, ((0, 32), (1, 4)))
    value_rows = bell_draw(keys[2], (TOKENS_A, RETENTION_HEADS * DV), 1.0, 6.0, ((0, 32), (1, 4)))
    gate_rows = bell_draw(keys[3], (TOKENS_A, RETENTION_HEADS * DV), 1.0, 6.0, ((0, 32), (1, 4)))
    log_decay = draw_log_decay(jax.random.fold_in(keys[16], 71), 0)
    out_proj = bell_draw(keys[5], (RETENTION_HEADS * DV, D), (RETENTION_HEADS * DV) ** -0.5, 0.125, ((0, 4),))
    moe_input = bell_draw(keys[6], (TOKENS_B, D), 1.0, 6.0, ((0, 128),))
    norm_gain = jnp.clip(1.0 + 0.18 * jax.random.normal(keys[7], (D,), jnp.float32), 0.1, 1.9)
    routing_keys = jax.random.split(jax.random.fold_in(keys[8], 1), TOKENS_B // TOK_B)
    routing_turns = jax.random.permutation(jax.random.fold_in(keys[8], 3), TOKENS_B // TOK_B)
    routing = jax.vmap(lambda own, number: deal_out(jax.random.fold_in(keys[8], 2), own, number, TOK_B, EXPERTS, TOP, CAP, 2))(routing_keys, routing_turns).reshape((TOKENS_B, TOP))
    route_weight = jnp.clip(0.2 + 0.8 * jax.random.uniform(keys[9], (TOKENS_B, TOP), jnp.float32) ** steps_of(keys[9], (TOKENS_B, TOP), ((0, 128),), -0.2, 0.2), 0.2, 1.0)
    expert_gate = bell_draw(keys[10], (EXPERTS, D, FF), D ** -0.5, 0.125, ((0, 128),))
    expert_up = bell_draw(keys[11], (EXPERTS, D, FF), D ** -0.5, 0.125, ((0, 128),))
    expert_down = bell_draw(keys[12], (EXPERTS, FF, D), FF ** -0.5, 0.25, ((0, 128),))
    shared_gate = bell_draw(keys[13], (D, SHARED_FF), D ** -0.5, 0.125)
    shared_up = bell_draw(keys[14], (D, SHARED_FF), D ** -0.5, 0.125)
    shared_down = bell_draw(keys[15], (SHARED_FF, D), SHARED_FF ** -0.5, 0.25)
    return {"query_rows": query_rows, "key_rows": key_rows, "value_rows": value_rows, "gate_rows": gate_rows, "log_decay": log_decay, "out_proj": out_proj, "moe_input": moe_input, "norm_gain": norm_gain, "routing": routing, "route_weight": route_weight, "expert_gate": expert_gate, "expert_up": expert_up, "expert_down": expert_down, "shared_gate": shared_gate, "shared_up": shared_up, "shared_down": shared_down}


EPS = 1e-06

def retention_all(query_rows, key_rows, value_rows, log_decay):
    n_blocks = TOKENS_A // BLOCK
    score_scale = DK ** (-0.5)
    q_blocks = query_rows.reshape(n_blocks, BLOCK, RETENTION_HEADS, DK)
    k_blocks = key_rows.reshape(n_blocks, BLOCK, RETENTION_HEADS, DK)
    v_blocks = value_rows.reshape(n_blocks, BLOCK, RETENTION_HEADS, DV)
    a_blocks = jnp.transpose(log_decay.reshape(RETENTION_HEADS, n_blocks, BLOCK), (1, 0, 2))
    causal = jnp.arange(BLOCK)[:, None] >= jnp.arange(BLOCK)[None, :]

    def advance(carried_state, block_in):
        q_blk, k_blk, v_blk, a_blk = block_in
        cum_decay = jnp.cumsum(a_blk, axis=1)
        block_count = cum_decay[:, -1]
        query_float = q_blk.astype(jnp.float32)
        key_float = k_blk.astype(jnp.float32)
        value_float = v_blk.astype(jnp.float32)
        retention_scores = jnp.einsum('gab,lab->agl', query_float, key_float)
        log_gap = jnp.where(causal[None], cum_decay[:, :, None] - cum_decay[:, None, :], 0.0)
        decay_mat = jnp.where(causal[None], jnp.exp(log_gap), 0.0)
        weight = (retention_scores * score_scale * decay_mat).astype(jnp.bfloat16)
        weight = lax.optimization_barrier(weight).astype(jnp.float32)
        inner_out = jnp.einsum('hnm,mhe->nhe', weight, value_float)
        state_low = lax.optimization_barrier(carried_state.astype(jnp.bfloat16)).astype(jnp.float32)
        cross_out = jnp.einsum('nhd,hde->nhe', query_float, state_low) * jnp.exp(cum_decay).T[:, :, None]
        decayed_key_rows = (key_float * score_scale * jnp.exp(block_count[None, :] - cum_decay.T)[:, :, None]).astype(jnp.bfloat16)
        decayed_key_rows = lax.optimization_barrier(decayed_key_rows).astype(jnp.float32)
        carried_state = carried_state * jnp.exp(block_count)[:, None, None] + jnp.einsum('czq,czy->zqy', decayed_key_rows, value_float)
        return (carried_state, inner_out + cross_out)
    initial = jnp.zeros((RETENTION_HEADS, DK, DV), jnp.float32)
    _, outputs = lax.scan(advance, initial, (q_blocks, k_blocks, v_blocks, a_blocks))
    return outputs.reshape(TOKENS_A, RETENTION_HEADS, DV)

def expert_apply(inputs, w_gate, w_up, w_down):
    gate_act = jnp.dot(inputs, w_gate, preferred_element_type=jnp.float32)
    up_act = jnp.dot(inputs, w_up, preferred_element_type=jnp.float32)
    hidden = (jax.nn.silu(gate_act) * up_act).astype(jnp.bfloat16)
    return jnp.dot(hidden, w_down, preferred_element_type=jnp.float32)

def reference(query_rows, key_rows, value_rows, gate_rows, log_decay, out_proj, moe_input, norm_gain, routing, route_weight, expert_gate, expert_up, expert_down, shared_gate, shared_up, shared_down):
    raw_out = retention_all(query_rows, key_rows, value_rows, log_decay)
    avg_out = lax.optimization_barrier(jnp.mean(raw_out, axis=-1, keepdims=True))
    spread = lax.optimization_barrier(jnp.mean(jnp.square(raw_out - avg_out), axis=-1, keepdims=True))
    normed = (raw_out - avg_out) * lax.rsqrt(spread + EPS)
    gate_act = jax.nn.silu(gate_rows.astype(jnp.float32).reshape(TOKENS_A, RETENTION_HEADS, DV))
    retained = (gate_act * normed).reshape(TOKENS_A, RETENTION_HEADS * DV).astype(jnp.bfloat16)
    group_cols = RETENTION_HEADS * DV // N_TP
    summed = jnp.zeros((TOKENS_A, D), jnp.float32)
    for group_idx in range(N_TP):
        lo_col = group_idx * group_cols
        partial_sum = jnp.dot(retained[:, lo_col:lo_col + group_cols], out_proj[lo_col:lo_col + group_cols], preferred_element_type=jnp.float32).astype(jnp.bfloat16)
        summed = summed + partial_sum.astype(jnp.float32)
    mixer_out = summed.astype(jnp.bfloat16)
    as_float = moe_input.astype(jnp.float32)
    moe_normed = (as_float * lax.rsqrt(lax.optimization_barrier(jnp.mean(as_float * as_float, axis=-1, keepdims=True)) + EPS) * norm_gain).astype(jnp.bfloat16)
    flat_route = routing.reshape(-1)
    flat_weight = route_weight.reshape(-1)
    bound_rows = N_EP * N_TP * CAP

    def visit(total_out, expert_idx):
        picked_rows = jnp.nonzero(flat_route == expert_idx, size=bound_rows, fill_value=0)[0].astype(jnp.int32)
        live_mask = (jnp.arange(bound_rows) < jnp.sum((flat_route == expert_idx).astype(jnp.int32))).astype(jnp.float32)
        token_idx = picked_rows // TOP
        result = expert_apply(moe_normed[token_idx], expert_gate[expert_idx], expert_up[expert_idx], expert_down[expert_idx])
        result = lax.optimization_barrier(result.astype(jnp.bfloat16)).astype(jnp.float32)
        scaled = result * (flat_weight[picked_rows] * live_mask)[:, None]
        return (total_out.at[token_idx].add(scaled), None)
    routed, _ = lax.scan(visit, jnp.zeros((TOKENS_B, D), jnp.float32), jnp.arange(N_EP * N_TP, dtype=jnp.int32))
    shared = expert_apply(moe_normed, shared_gate, shared_up, shared_down)
    moe_out = (routed + shared).astype(jnp.bfloat16)
    return (mixer_out, moe_out)
```

```python
import functools

import jax
import jax.numpy as jnp
from jax import lax
from jax.experimental import pallas as pl
from jax.experimental.pallas import tpu as pltpu
from jax.sharding import Mesh
from jax.sharding import PartitionSpec as P


DK = 128
DV = 256
BLOCK = 128
CAP = 8
NOTE = 16
EP = ("ep_0", "ep_1", "ep_2")
EP_TP = ("ep_0", "ep_1", "ep_2", "tp")
EPS = 1e-06
SCALE = DK ** (-0.5)
F32 = jnp.float32
BF16 = jnp.bfloat16
HIGHEST = lax.Precision.HIGHEST


def iota(shape, dim):
    return lax.broadcasted_iota(jnp.int32, shape, dim)


def dot(a, b):
    return jnp.dot(a, b, preferred_element_type=F32)


def dot_nt(a, b, precision=None):
    return lax.dot_general(
        a, b, (((1,), (1,)), ((), ())), preferred_element_type=F32, precision=precision
    )


def dot_tn(a, b):
    return lax.dot_general(a, b, (((0,), (0,)), ((), ())), preferred_element_type=F32)


def silu(v):
    return v / (1.0 + jnp.exp(-v))


def block_sums(a, inclusive):
    t, s = iota((BLOCK, BLOCK), 0), iota((BLOCK, BLOCK), 1)
    pick = jnp.where(s <= t if inclusive else s > t, 1.0, 0.0)
    return dot_nt(pick, a, HIGHEST)


def write_message(ref, h, state, total):
    whole = jnp.broadcast_to(total, (NOTE, DV))
    high = whole.astype(BF16).astype(F32)
    middle = (whole - high).astype(BF16).astype(F32)
    row = iota((NOTE, DV), 0)
    note = jnp.where(row == 0, high, jnp.where(row == 1, middle, whole - high - middle))
    ref[h, :DK] = state.astype(BF16)
    ref[h, DK:] = note.astype(BF16)


def read_message(ref, k, h):
    note = ref[k, h, DK:].astype(F32)
    return ref[k, h, :DK].astype(F32), note[0:1] + note[1:2] + note[2:3]


def end_state_body(k_ref, v_ref, a_ref, out_ref, state, total):
    step = pl.program_id(0)

    @pl.when(step == 0)
    def _():
        state[...] = jnp.zeros_like(state)
        total[...] = jnp.zeros_like(total)

    n_heads = a_ref.shape[0]
    for b in range(k_ref.shape[0] // BLOCK):
        rows = pl.ds(b * BLOCK, BLOCK)
        a = a_ref[:, rows]
        left = block_sums(a, False)
        gone = jnp.sum(a, axis=1, keepdims=True)
        for h in range(n_heads):
            k = k_ref[rows, h * DK : (h + 1) * DK].astype(F32)
            v = v_ref[rows, h * DV : (h + 1) * DV]
            k = (k * (SCALE * jnp.exp(left[:, h : h + 1]))).astype(BF16)
            gone_h = gone[h : h + 1, :]
            state[h] = state[h] * jnp.exp(gone_h) + dot_tn(k, v)
            total[h] = total[h] + gone_h

    @pl.when(step == pl.num_programs(0) - 1)
    def _():
        for h in range(n_heads):
            write_message(out_ref, h, state[h], total[h, 0:1, 0:1])


def end_state(key_rows, value_rows, log_decay):
    n_rows, n_heads = key_rows.shape[0], log_decay.shape[0]
    tile = min(512, n_rows)
    return pl.pallas_call(
        end_state_body,
        grid=(n_rows // tile,),
        in_specs=[
            pl.BlockSpec((tile, n_heads * DK), lambda i: (i, 0)),
            pl.BlockSpec((tile, n_heads * DV), lambda i: (i, 0)),
            pl.BlockSpec((n_heads, tile), lambda i: (0, i)),
        ],
        out_specs=pl.BlockSpec((n_heads, DK + NOTE, DV), lambda i: (0, 0, 0)),
        out_shape=jax.ShapeDtypeStruct((n_heads, DK + NOTE, DV), BF16),
        scratch_shapes=[
            pltpu.VMEM((n_heads, DK, DV), F32),
            pltpu.VMEM((n_heads, 8, 128), F32),
        ],
        cost_estimate=pl.CostEstimate(
            flops=2 * n_rows * n_heads * DK * DV, bytes_accessed=4 << 20, transcendentals=0
        ),
        name="end_state",
    )(key_rows, value_rows, log_decay)


def join_body(axis, peers, last, *refs):
    messages, before_ref, refs = refs[:peers], refs[peers], refs[peers + 1 :]
    ordered = refs[-1]
    me = lax.axis_index(axis)
    for d in range(peers):
        ordered[(me - d + peers) % peers] = messages[d][...]
    for h in range(before_ref.shape[0]):
        running, ahead = jnp.zeros((DK, DV), F32), jnp.zeros((DK, DV), F32)
        total, ahead_total = jnp.zeros((1, DV), F32), jnp.zeros((1, DV), F32)
        for k in range(peers):
            ahead = jnp.where(k == me, running, ahead)
            ahead_total = jnp.where(k == me, total, ahead_total)
            if last and k == peers - 1:
                break
            state, gone = read_message(ordered, k, h)
            running = running * jnp.exp(gone) + state
            total = total + gone
        gone = before_ref[h, DK : DK + 1]
        refs[0][h, :DK] = ahead * jnp.exp(gone) + before_ref[h, :DK]
        refs[0][h, DK:] = jnp.broadcast_to(ahead_total + gone, (8, DV))
        if not last:
            write_message(refs[1], h, running, total)


def join(axis, messages, before, last):
    peers = len(messages)
    n_heads = messages[0].shape[0]
    out = [jax.ShapeDtypeStruct((n_heads, DK + 8, DV), F32)]
    if not last:
        out.append(jax.ShapeDtypeStruct(messages[0].shape, BF16))
    return pl.pallas_call(
        functools.partial(join_body, axis, peers, last),
        out_shape=out,
        scratch_shapes=[pltpu.VMEM((peers,) + messages[0].shape, BF16)],
        cost_estimate=pl.CostEstimate(flops=1 << 22, bytes_accessed=2 << 20, transcendentals=0),
        name="join",
    )(*messages, before)


def shift(x, axis, d):
    peers = lax.axis_size(axis)
    return lax.ppermute(x, axis, [(k, (k + d) % peers) for k in range(peers)])


def all_shifts(x, axis):
    return [x] + [shift(x, axis, d) for d in range(1, lax.axis_size(axis))]


def mixer_body(q_ref, k_ref, v_ref, g_ref, a_ref, first_ref, out_ref, state):
    @pl.when(pl.program_id(0) == 0)
    def _():
        state[...] = first_ref[:, :DK]

    n_heads = a_ref.shape[0]
    t, m = iota((BLOCK, BLOCK), 0), iota((BLOCK, BLOCK), 1)
    causal = t >= m
    upto = jnp.where(t <= m, 1.0, 0.0)
    for b in range(q_ref.shape[0] // BLOCK):
        rows = pl.ds(b * BLOCK, BLOCK)
        a = a_ref[:, rows]
        down = block_sums(a, True)
        across = jnp.dot(a, upto, preferred_element_type=F32, precision=HIGHEST)
        for h in range(n_heads):
            q = q_ref[rows, h * DK : (h + 1) * DK]
            k = k_ref[rows, h * DK : (h + 1) * DK]
            v = v_ref[rows, h * DV : (h + 1) * DV]
            gate = g_ref[rows, h * DV : (h + 1) * DV].astype(F32)
            col, row = down[:, h : h + 1], across[h : h + 1, :]
            whole = row[:, BLOCK - 1 : BLOCK]
            decay = jnp.where(causal, jnp.exp(jnp.where(causal, col - row, 0.0)), 0.0)
            weight = (dot_nt(q, k) * SCALE * decay).astype(BF16)
            before = state[h]
            raw = dot(weight, v) + dot(q, before.astype(BF16)) * jnp.exp(col)
            faded = (k.astype(F32) * (SCALE * jnp.exp(whole - col))).astype(BF16)
            state[h] = before * jnp.exp(whole) + dot_tn(faded, v)
            centered = raw - jnp.mean(raw, axis=1, keepdims=True)
            spread = jnp.mean(centered * centered, axis=1, keepdims=True)
            normed = centered * lax.rsqrt(spread + EPS)
            out_ref[rows, h * DV : (h + 1) * DV] = (silu(gate) * normed).astype(BF16)


def mixer(query_rows, key_rows, value_rows, gate_rows, log_decay, incoming):
    n_rows, n_heads = query_rows.shape[0], log_decay.shape[0]
    tile = min(256, n_rows)
    return pl.pallas_call(
        mixer_body,
        grid=(n_rows // tile,),
        in_specs=[
            pl.BlockSpec((tile, n_heads * DK), lambda i: (i, 0)),
            pl.BlockSpec((tile, n_heads * DK), lambda i: (i, 0)),
            pl.BlockSpec((tile, n_heads * DV), lambda i: (i, 0)),
            pl.BlockSpec((tile, n_heads * DV), lambda i: (i, 0)),
            pl.BlockSpec((n_heads, tile), lambda i: (0, i)),
            pl.BlockSpec((n_heads, DK + 8, DV), lambda i: (0, 0, 0)),
        ],
        out_specs=pl.BlockSpec((tile, n_heads * DV), lambda i: (i, 0)),
        out_shape=jax.ShapeDtypeStruct((n_rows, n_heads * DV), BF16),
        scratch_shapes=[pltpu.VMEM((n_heads, DK, DV), F32)],
        cost_estimate=pl.CostEstimate(
            flops=12 * n_rows * n_heads * DK * DV, bytes_accessed=8 << 20, transcendentals=0
        ),
        name="mixer",
    )(query_rows, key_rows, value_rows, gate_rows, log_decay, incoming)


def project_body(*refs):
    heads, weights, out_ref, lhs, rhs, sems = refs[:4], refs[4:20], *refs[20:]
    x, core = lax.axis_index("tp"), lax.axis_index("ep_2")
    up, out_of = lax.axis_index("ep_1"), lax.axis_index("ep_0")
    copies = [pltpu.make_async_copy(heads[0].at[x], lhs.at[0], sems.at[16])]
    for d in range(1, 4):
        copies.append(pltpu.make_async_copy(heads[d], lhs.at[d], sems.at[16 + d]))
    for part in range(4):
        me = up if part % 2 == 0 else out_of
        for d in range(4):
            n = part * 4 + d
            to = rhs.at[part, :, (me - d + 4) % 4]
            copies.append(pltpu.make_async_copy(weights[n], to, sems.at[n]))
    for copy in copies:
        copy.start()
    for copy in copies[:4]:
        copy.wait()
    _, width = lhs.shape[1:]
    fine = rhs.shape[-1]
    for part in range(4):
        for d in range(4):
            copies[4 + part * 4 + d].wait()
        total = dot(lhs[0], rhs[part, 0].reshape(width, fine))
        for d in range(1, 4):
            total = total + dot(lhs[d], rhs[part, d].reshape(width, fine))
        whose = core if part < 2 else 1 - core
        at = pl.multiple_of((part % 2) * 2 * fine + whose * fine, fine)
        out_ref[:, pl.ds(at, fine)] = total.astype(BF16)


def project(retained, received, own, other):
    groups, n_rows, width = retained.shape
    fine = own[0].shape[-1]
    arrays = [retained, *received, *own, *other]
    return pl.pallas_call(
        project_body,
        in_specs=[pl.BlockSpec(memory_space=pl.ANY)] * len(arrays),
        out_shape=jax.ShapeDtypeStruct((n_rows, 4 * fine), BF16),
        scratch_shapes=[
            pltpu.VMEM((groups, n_rows, width), BF16),
            pltpu.VMEM((4, groups, 4) + own[0].shape[1:], BF16),
            pltpu.SemaphoreType.DMA((20,)),
        ],
        cost_estimate=pl.CostEstimate(
            flops=8 * n_rows * groups * width * fine, bytes_accessed=12 << 20, transcendentals=0
        ),
        name="project",
    )(*arrays)


def gather_projection(out_proj):
    n_rows, width = out_proj.shape
    core = lax.axis_index("ep_2")
    rows, cols = n_rows // 4, width // 4
    left = lax.dynamic_slice(
        out_proj, (lax.axis_index("ep_1") * rows, core * cols), (rows, cols)
    )
    right = lax.dynamic_slice(
        out_proj, (lax.axis_index("ep_0") * rows, (2 + core) * cols), (rows, cols)
    )
    over_x = all_shifts(jnp.stack([left, right]), "tp")
    own = all_shifts(jnp.stack([part[0] for part in over_x]), "ep_1")
    own = own + all_shifts(jnp.stack([part[1] for part in over_x]), "ep_0")
    other = [shift(part, "ep_2", 1) for part in own]
    return own, other


def dispatch_body(x_ref, gain_ref, route_ref, weight_ref, normed_ref, out_ref, high_ref, low_ref):
    x = x_ref[...].astype(F32)
    mean = jnp.mean(x * x, axis=1, keepdims=True)
    normed = (x * lax.rsqrt(mean + EPS) * gain_ref[...]).astype(BF16)
    normed_ref[...] = normed
    n_tokens, n_visits = route_ref.shape
    n_slots = out_ref.shape[0]
    experts = n_slots // CAP
    route, weight = route_ref[...], weight_ref[...]
    lane = iota((n_tokens, experts), 1)
    named = jnp.zeros((n_tokens, experts), F32)
    weighed = jnp.zeros((n_tokens, experts), F32)
    for k in range(n_visits):
        hit = route[:, k : k + 1] == lane
        named = jnp.where(hit, 1.0, named)
        weighed = jnp.where(hit, weight[:, k : k + 1], weighed)
    earlier = iota((n_tokens, n_tokens), 0) > iota((n_tokens, n_tokens), 1)
    rank = dot(jnp.where(earlier, 1.0, 0.0).astype(BF16), named.astype(BF16))
    rank = jnp.where(named > 0.0, rank, float(CAP))
    spread = jnp.where(iota((experts, n_slots), 1) // CAP == iota((experts, n_slots), 0), 1.0, 0.0)
    spread = spread.astype(BF16)
    place = (iota((n_tokens, n_slots), 1) % CAP).astype(F32)
    here = dot(rank.astype(BF16), spread) == place
    high = weighed.astype(BF16)
    low = (weighed - high.astype(F32)).astype(BF16)
    high_ref[...] = jnp.where(here, dot(high, spread), 0.0).astype(BF16)
    low_ref[...] = jnp.where(here, dot(low, spread), 0.0).astype(BF16)
    pick = jnp.where(here, 1.0, 0.0).astype(BF16)
    out_ref[...] = dot_tn(pick, normed).astype(BF16)


def dispatch(moe_input, norm_gain, routing, route_weight, experts):
    n_tokens, width = moe_input.shape
    n_slots = experts * CAP
    return pl.pallas_call(
        dispatch_body,
        out_shape=(
            jax.ShapeDtypeStruct((n_tokens, width), BF16),
            jax.ShapeDtypeStruct((n_slots, width), BF16),
            jax.ShapeDtypeStruct((n_tokens, n_slots), BF16),
            jax.ShapeDtypeStruct((n_tokens, n_slots), BF16),
        ),
        cost_estimate=pl.CostEstimate(
            flops=2 * n_tokens * n_slots * width, bytes_accessed=6 << 20, transcendentals=0
        ),
        name="dispatch",
    )(moe_input, norm_gain.reshape(1, width), routing, route_weight)


def expert_body(x_ref, gate_ref, up_ref, down_ref, out_ref):
    x = x_ref[...]
    hidden = (silu(dot(x, gate_ref[...])) * dot(x, up_ref[...])).astype(BF16)
    out_ref[...] = dot(hidden, down_ref[...]).astype(out_ref.dtype)


def expert_apply(rows, w_gate, w_up, w_down, dtype):
    n_rows, width = rows.shape
    hidden = w_gate.shape[1]
    tile = min(256, n_rows)
    return pl.pallas_call(
        expert_body,
        grid=(n_rows // tile,),
        in_specs=[
            pl.BlockSpec((tile, width), lambda i: (i, 0)),
            pl.BlockSpec((width, hidden), lambda i: (0, 0)),
            pl.BlockSpec((width, hidden), lambda i: (0, 0)),
            pl.BlockSpec((hidden, width), lambda i: (0, 0)),
        ],
        out_specs=pl.BlockSpec((tile, width), lambda i: (i, 0)),
        out_shape=jax.ShapeDtypeStruct((n_rows, width), dtype),
        cost_estimate=pl.CostEstimate(
            flops=6 * n_rows * width * hidden, bytes_accessed=14 << 20, transcendentals=0
        ),
        name="expert",
    )(rows, w_gate, w_up, w_down)


def combine_body(high_ref, low_ref, rows_ref, shared_ref, out_ref):
    rows = rows_ref[...]
    total = dot(high_ref[...], rows) + dot(low_ref[...], rows) + shared_ref[...]
    out_ref[...] = total.astype(BF16)


def combine(high, low, rows, shared):
    n_tokens, n_slots = high.shape
    width = rows.shape[1]
    tile = width // 4
    return pl.pallas_call(
        combine_body,
        grid=(width // tile,),
        in_specs=[
            pl.BlockSpec((n_tokens, n_slots), lambda i: (0, 0)),
            pl.BlockSpec((n_tokens, n_slots), lambda i: (0, 0)),
            pl.BlockSpec((n_slots, tile), lambda i: (0, i)),
            pl.BlockSpec((n_tokens, tile), lambda i: (0, i)),
        ],
        out_specs=pl.BlockSpec((n_tokens, tile), lambda i: (0, i)),
        out_shape=jax.ShapeDtypeStruct((n_tokens, width), BF16),
        cost_estimate=pl.CostEstimate(
            flops=4 * n_tokens * n_slots * width, bytes_accessed=6 << 20, transcendentals=0
        ),
        name="combine",
    )(high, low, rows, shared)


def exchange(x, axes):
    return lax.all_to_all(x, axes, split_axis=0, concat_axis=0, tiled=True)


def local(
    query_rows,
    key_rows,
    value_rows,
    gate_rows,
    log_decay,
    out_proj,
    moe_input,
    norm_gain,
    routing,
    route_weight,
    expert_gate,
    expert_up,
    expert_down,
    shared_gate,
    shared_up,
    shared_down,
):
    n_rows = query_rows.shape[0]
    width = moe_input.shape[1]
    tp = lax.axis_size("tp")
    experts = lax.axis_size(EP) * tp

    normed, outgoing, high, low = dispatch(moe_input, norm_gain, routing, route_weight, experts)
    received = exchange(outgoing.reshape(experts, CAP, width), EP_TP)

    message = end_state(key_rows, value_rows, log_decay)
    before = jnp.zeros((message.shape[0], DK + 8, DV), F32)
    for axis in reversed(EP):
        messages = all_shifts(message, axis)
        before, *message = join(axis, messages, before, axis == EP[0])
        message = message[0] if message else None

    own, other = gather_projection(out_proj)

    shared = expert_apply(normed, shared_gate, shared_up, shared_down, F32)
    retained = mixer(query_rows, key_rows, value_rows, gate_rows, log_decay, before)
    retained = retained.reshape(tp, n_rows // tp, -1)
    place = lax.axis_index("tp")
    heads = []
    for d in range(1, tp):
        block = lax.dynamic_index_in_dim(retained, (place + d) % tp, keepdims=False)
        heads.append(shift(block, "tp", d))

    served = expert_apply(
        received.reshape(-1, width), expert_gate[0], expert_up[0], expert_down[0], BF16
    )
    returned = exchange(served.reshape(experts, CAP, width), EP_TP)

    mixer_out = project(retained, heads, own, other)
    moe_out = combine(high, low, returned.reshape(-1, width), shared)
    return (mixer_out, moe_out)


def solution(mesh):
    split = Mesh(mesh.devices.reshape(4, 4, 2, mesh.shape["tp"]), ("ep_0", "ep_1", "ep_2", "tp"))
    return jax.shard_map(
        local,
        mesh=split,
        in_specs=(
            P(EP, "tp"),
            P(EP, "tp"),
            P(EP, "tp"),
            P(EP, "tp"),
            P("tp", EP),
            P("tp", None),
            P(EP_TP, None),
            P(),
            P(EP_TP, None),
            P(EP_TP, None),
            P(EP_TP, None, None),
            P(EP_TP, None, None),
            P(EP_TP, None, None),
            P(),
            P(),
            P(),
        ),
        out_specs=(P(EP_TP, None), P(EP_TP, None)),
        check_vma=False,
    )
```

```python
import jax
import jax.numpy as jnp
from jax import lax
from jax.experimental import pallas as pl
from jax.experimental.pallas import tpu as pltpu
from jax.sharding import Mesh
from jax.sharding import PartitionSpec as P


DK = 128
DV = 256
BLOCK = 128
CAP = 8
NOTE = 16
EP = ("ep_0", "ep_1", "ep_2")
EP_TP = ("ep_0", "ep_1", "ep_2", "tp")
EPS = 1e-06
SCALE = DK ** (-0.5)
F32 = jnp.float32
BF16 = jnp.bfloat16


def iota(shape, dim):
    return lax.broadcasted_iota(jnp.int32, shape, dim)


def dot(a, b):
    return jnp.dot(a, b, preferred_element_type=F32)


def dot_nt(a, b):
    return lax.dot_general(a, b, (((1,), (1,)), ((), ())), preferred_element_type=F32)


def dot_tn(a, b):
    return lax.dot_general(a, b, (((0,), (0,)), ((), ())), preferred_element_type=F32)


def silu(v):
    return v / (1.0 + jnp.exp(-v))


def thirds(a):
    high = a.astype(BF16)
    rest = a - high.astype(F32)
    middle = rest.astype(BF16)
    return high, middle, (rest - middle.astype(F32)).astype(BF16)


def sums_down(pick, a):
    return sum(dot_nt(pick, part) for part in thirds(a))


def sums_across(a, pick):
    return sum(dot(part, pick) for part in thirds(a))


def end_state_body(k_ref, v_ref, a_ref, out_ref, state, total):
    step = pl.program_id(0)

    @pl.when(step == 0)
    def _():
        state[...] = jnp.zeros_like(state)
        total[...] = jnp.zeros_like(total)

    n_heads = a_ref.shape[0]
    n_blocks = k_ref.shape[0] // BLOCK
    after = iota((BLOCK, BLOCK), 1) > iota((BLOCK, BLOCK), 0)
    pick = jnp.where(after, 1.0, 0.0).astype(BF16)
    later = jnp.zeros((n_heads, 1), F32)
    keys = [[] for _ in range(n_heads)]
    for b in reversed(range(n_blocks)):
        rows = pl.ds(b * BLOCK, BLOCK)
        a = a_ref[:, rows]
        left = sums_down(pick, a)
        for h in range(n_heads):
            k = k_ref[rows, h * DK : (h + 1) * DK].astype(F32)
            fade = SCALE * jnp.exp(left[:, h : h + 1] + later[h : h + 1, :])
            keys[h].insert(0, (k * fade).astype(BF16))
        later = later + jnp.sum(a, axis=1, keepdims=True)
    for h in range(n_heads):
        gone = later[h : h + 1, :]
        added = dot_tn(jnp.concatenate(keys[h], axis=0), v_ref[:, h * DV : (h + 1) * DV])
        state[h] = state[h] * jnp.exp(gone) + added
        total[h] = total[h] + gone

    @pl.when(step == pl.num_programs(0) - 1)
    def _():
        parts = DK // 8
        for h in range(n_heads):
            whole = jnp.broadcast_to(total[h, 0:1, 0:1], (8, DV))
            high, middle, low = (part.astype(F32) for part in thirds(whole))
            row = iota((8, DV), 0)
            note = jnp.where(row == 0, high, jnp.where(row == 1, middle, low))
            note = jnp.broadcast_to(note[None], (parts, 8, DV))
            both = jnp.concatenate([state[h].reshape(parts, 8, DV), note], axis=1)
            out_ref[h * parts : (h + 1) * parts] = both.astype(BF16)


def end_state(key_rows, value_rows, log_decay):
    n_rows, n_heads = key_rows.shape[0], log_decay.shape[0]
    tile = min(512, n_rows)
    parts = n_heads * DK // 8
    return pl.pallas_call(
        end_state_body,
        grid=(n_rows // tile,),
        in_specs=[
            pl.BlockSpec((tile, n_heads * DK), lambda i: (i, 0)),
            pl.BlockSpec((tile, n_heads * DV), lambda i: (i, 0)),
            pl.BlockSpec((n_heads, tile), lambda i: (0, i)),
        ],
        out_specs=pl.BlockSpec((parts, 16, DV), lambda i: (0, 0, 0)),
        out_shape=jax.ShapeDtypeStruct((parts, 16, DV), BF16),
        scratch_shapes=[
            pltpu.VMEM((n_heads, DK, DV), F32),
            pltpu.VMEM((n_heads, 8, 128), F32),
        ],
        cost_estimate=pl.CostEstimate(
            flops=2 * n_rows * n_heads * DK * DV, bytes_accessed=4 << 20, transcendentals=0
        ),
        name="end_state",
    )(key_rows, value_rows, log_decay)


def prefix_body(in_ref, out_ref):
    before = jnp.zeros((8, DV), F32)
    for j in range(in_ref.shape[0]):
        out_ref[j] = before.astype(BF16)
        both = in_ref[j].astype(F32)
        total = both[8:9] + both[9:10] + both[10:11]
        before = before * jnp.exp(total) + both[0:8]


def prefixes(pieces):
    return pl.pallas_call(
        prefix_body,
        out_shape=jax.ShapeDtypeStruct((pieces.shape[0], 8, DV), BF16),
        name="prefixes",
    )(pieces)


def shift(x, axis, d):
    peers = lax.axis_size(axis)
    return lax.ppermute(x, axis, [(k, (k + d) % peers) for k in range(peers)])


def all_shifts(x, axis):
    return [x] + [shift(x, axis, d) for d in range(1, lax.axis_size(axis))]


def mixer_body(q_ref, k_ref, v_ref, g_ref, a_ref, first_ref, out_ref, state):
    @pl.when(pl.program_id(0) == 0)
    def _():
        state[...] = first_ref[...].astype(F32).reshape(state.shape)

    n_heads = a_ref.shape[0]
    t, m = iota((BLOCK, BLOCK), 0), iota((BLOCK, BLOCK), 1)
    causal = t >= m
    upto = jnp.where(t <= m, 1.0, 0.0).astype(BF16)
    downto = jnp.where(causal, 1.0, 0.0).astype(BF16)
    for b in range(q_ref.shape[0] // BLOCK):
        rows = pl.ds(b * BLOCK, BLOCK)
        a = a_ref[:, rows]
        down = sums_down(downto, a)
        across = sums_across(a, upto)
        for h in range(n_heads):
            q = q_ref[rows, h * DK : (h + 1) * DK]
            k = k_ref[rows, h * DK : (h + 1) * DK]
            v = v_ref[rows, h * DV : (h + 1) * DV]
            gate = g_ref[rows, h * DV : (h + 1) * DV].astype(F32)
            col, row = down[:, h : h + 1], across[h : h + 1, :]
            whole = row[:, BLOCK - 1 : BLOCK]
            decay = jnp.where(causal, jnp.exp(jnp.where(causal, col - row, 0.0)), 0.0)
            weight = (dot_nt(q, k) * SCALE * decay).astype(BF16)
            before = state[h]
            raw = dot(weight, v) + dot(q, before.astype(BF16)) * jnp.exp(col)
            faded = (k.astype(F32) * (SCALE * jnp.exp(whole - col))).astype(BF16)
            state[h] = before * jnp.exp(whole) + dot_tn(faded, v)
            centered = raw - jnp.mean(raw, axis=1, keepdims=True)
            spread = jnp.mean(centered * centered, axis=1, keepdims=True)
            normed = centered * lax.rsqrt(spread + EPS)
            out_ref[rows, h * DV : (h + 1) * DV] = (silu(gate) * normed).astype(BF16)


def mixer(query_rows, key_rows, value_rows, gate_rows, log_decay, incoming):
    n_rows, n_heads = query_rows.shape[0], log_decay.shape[0]
    tile = min(256, n_rows)
    return pl.pallas_call(
        mixer_body,
        grid=(n_rows // tile,),
        in_specs=[
            pl.BlockSpec((tile, n_heads * DK), lambda i: (i, 0)),
            pl.BlockSpec((tile, n_heads * DK), lambda i: (i, 0)),
            pl.BlockSpec((tile, n_heads * DV), lambda i: (i, 0)),
            pl.BlockSpec((tile, n_heads * DV), lambda i: (i, 0)),
            pl.BlockSpec((n_heads, tile), lambda i: (0, i)),
            pl.BlockSpec((n_heads * DK, DV), lambda i: (0, 0)),
        ],
        out_specs=pl.BlockSpec((tile, n_heads * DV), lambda i: (i, 0)),
        out_shape=jax.ShapeDtypeStruct((n_rows, n_heads * DV), BF16),
        scratch_shapes=[pltpu.VMEM((n_heads, DK, DV), F32)],
        cost_estimate=pl.CostEstimate(
            flops=12 * n_rows * n_heads * DK * DV, bytes_accessed=8 << 20, transcendentals=0
        ),
        name="mixer",
    )(query_rows, key_rows, value_rows, gate_rows, log_decay, incoming)


def project_body(*refs):
    heads, whole, own, other, out_ref, lhs, rhs, sems = (
        refs[:4],
        refs[4],
        refs[5:8],
        refs[8:11],
        *refs[11:],
    )
    x, core = lax.axis_index("tp"), lax.axis_index("ep_2")
    half = rhs.shape[-1]
    pairs = [(heads[0].at[x], lhs.at[0])]
    for d in range(1, 4):
        pairs.append((heads[d], lhs.at[d]))
    for side in range(2):
        pairs.append((whole.at[:, side * half : (side + 1) * half], rhs.at[0, side]))
    for d in range(1, 4):
        pairs.append((own[d - 1], rhs.at[d, core]))
        pairs.append((other[d - 1], rhs.at[d, 1 - core]))
    copies = [
        pltpu.make_async_copy(source, target, sems.at[n])
        for n, (source, target) in enumerate(pairs)
    ]
    for copy in copies:
        copy.start()
    for copy in copies:
        copy.wait()
    fine = half // 2
    for side in range(2):
        for part in range(2):
            at = slice(part * fine, (part + 1) * fine)
            total = dot(lhs[0], rhs[0, side, :, at])
            for d in range(1, 4):
                total = total + dot(lhs[d], rhs[d, side, :, at])
            start = side * half + part * fine
            out_ref[:, start : start + fine] = total.astype(BF16)


def project(retained, received, whole, own, other):
    groups, n_rows, width = retained.shape
    half = whole.shape[1] // 2
    arrays = [retained, *received, whole, *own, *other]
    return pl.pallas_call(
        project_body,
        in_specs=[pl.BlockSpec(memory_space=pl.ANY)] * len(arrays),
        out_shape=jax.ShapeDtypeStruct((n_rows, 2 * half), BF16),
        scratch_shapes=[
            pltpu.VMEM((groups, n_rows, width), BF16),
            pltpu.VMEM((groups, 2, width, half), BF16),
            pltpu.SemaphoreType.DMA((12,)),
        ],
        cost_estimate=pl.CostEstimate(
            flops=4 * n_rows * groups * width * half, bytes_accessed=12 << 20, transcendentals=0
        ),
        name="project",
    )(*arrays)


def gather_projection(out_proj):
    n_rows, width = out_proj.shape
    half = width // 2
    mine = lax.dynamic_slice(out_proj, (0, lax.axis_index("ep_2") * half), (n_rows, half))
    own = all_shifts(mine, "tp")[1:]
    other = [shift(part, "ep_2", 1) for part in own]
    return own, other


def norm_body(x_ref, gain_ref, route_ref, out_ref):
    x = x_ref[...].astype(F32)
    n_tokens = x.shape[0]
    mean = jnp.mean(x * x, axis=1, keepdims=True)
    out_ref[:n_tokens] = (x * lax.rsqrt(mean + EPS) * gain_ref[...]).astype(BF16)
    row = iota((NOTE, n_tokens), 0)
    note = jnp.zeros((NOTE, n_tokens), F32)
    for k in range(route_ref.shape[0]):
        note = jnp.where(row == k, route_ref[k : k + 1].astype(F32), note)
    out_ref[n_tokens:, :n_tokens] = note.astype(BF16)
    rest = (NOTE, x.shape[1] - n_tokens)
    out_ref[n_tokens:, n_tokens:] = jnp.zeros(rest, BF16)


def norm(moe_input, norm_gain, routes):
    n_tokens, width = moe_input.shape
    return pl.pallas_call(
        norm_body,
        out_shape=jax.ShapeDtypeStruct((n_tokens + NOTE, width), BF16),
        name="norm",
    )(moe_input, norm_gain.reshape(1, width), routes)


def ranked(hits, n_tokens):
    earlier = iota((n_tokens, n_tokens), 0) < iota((n_tokens, n_tokens), 1)
    rank = dot(hits.astype(BF16), jnp.where(earlier, 1.0, 0.0).astype(BF16))
    return jnp.where(hits > 0.0, rank, float(CAP)).astype(BF16)


def dispatch_body(*refs):
    messages, out_ref = refs[:-1], refs[-1]
    groups = len(messages)
    n_slots = out_ref.shape[0]
    each = groups * CAP
    experts = n_slots // each
    n_tokens = messages[0].shape[0] - NOTE
    x = lax.axis_index("tp")
    expert = (iota((experts, n_tokens), 0) * groups + x).astype(F32)
    spread = jnp.where(iota((n_slots, experts), 0) // each == iota((n_slots, experts), 1), 1.0, 0.0)
    spread = spread.astype(BF16)
    slot = iota((n_slots, n_tokens), 0)
    place = (slot % CAP).astype(F32)
    block = (slot // CAP) % groups
    picks = []
    for d in range(groups):
        named = messages[d][n_tokens:, :n_tokens].astype(F32)
        hits = jnp.zeros((experts, n_tokens), F32)
        for k in range(4):
            hits = jnp.where(named[k : k + 1] == expert, 1.0, hits)
        here = dot(spread, ranked(hits, n_tokens)) == place
        here = here & (block == (x - d + groups) % groups)
        picks.append(jnp.where(here, 1.0, 0.0).astype(BF16))
    for d in range(0, groups, 2):
        pick = jnp.concatenate([picks[d], picks[d + 1]], axis=1)
        rows = jnp.concatenate([messages[d][:n_tokens], messages[d + 1][:n_tokens]], axis=0)
        part = dot(pick, rows)
        total = part if d == 0 else total + part
    out_ref[...] = total.astype(BF16)


def dispatch(messages, n_slots):
    width = messages[0].shape[1]
    return pl.pallas_call(
        dispatch_body,
        out_shape=jax.ShapeDtypeStruct((n_slots, width), BF16),
        cost_estimate=pl.CostEstimate(
            flops=1024 * n_slots * width, bytes_accessed=6 << 20, transcendentals=0
        ),
        name="dispatch",
    )(*messages)


def weights_body(route_ref, weight_ref, high_ref, low_ref):
    n_visits, n_tokens = route_ref.shape
    n_slots = high_ref.shape[0]
    experts = n_slots // CAP
    expert = iota((experts, n_tokens), 0)
    hits = jnp.zeros((experts, n_tokens), F32)
    weighed = jnp.zeros((experts, n_tokens), F32)
    for k in range(n_visits):
        hit = route_ref[k : k + 1] == expert
        hits = jnp.where(hit, 1.0, hits)
        weighed = jnp.where(hit, weight_ref[k : k + 1], weighed)
    spread = jnp.where(iota((n_slots, experts), 0) // CAP == iota((n_slots, experts), 1), 1.0, 0.0)
    spread = spread.astype(BF16)
    place = (iota((n_slots, n_tokens), 0) % CAP).astype(F32)
    here = dot(spread, ranked(hits, n_tokens)) == place
    high = weighed.astype(BF16)
    low = (weighed - high.astype(F32)).astype(BF16)
    high_ref[...] = jnp.where(here, dot(spread, high), 0.0).astype(BF16)
    low_ref[...] = jnp.where(here, dot(spread, low), 0.0).astype(BF16)


def slot_weights(routes, route_weights, n_slots):
    n_tokens = routes.shape[1]
    return pl.pallas_call(
        weights_body,
        out_shape=[jax.ShapeDtypeStruct((n_slots, n_tokens), BF16)] * 2,
        cost_estimate=pl.CostEstimate(flops=1 << 27, bytes_accessed=1 << 20, transcendentals=0),
        name="weights",
    )(routes, route_weights)


def expert_body(x_ref, gate_ref, up_ref, down_ref, out_ref):
    x = x_ref[...]
    hidden = (silu(dot(x, gate_ref[...])) * dot(x, up_ref[...])).astype(BF16)
    out_ref[...] = dot(hidden, down_ref[...]).astype(out_ref.dtype)


def expert_apply(rows, w_gate, w_up, w_down, dtype, n_rows=None):
    n_rows, width = n_rows or rows.shape[0], rows.shape[1]
    hidden = w_gate.shape[1]
    tile = min(256, n_rows)
    return pl.pallas_call(
        expert_body,
        grid=(n_rows // tile,),
        in_specs=[
            pl.BlockSpec((tile, width), lambda i: (i, 0)),
            pl.BlockSpec((width, hidden), lambda i: (0, 0)),
            pl.BlockSpec((width, hidden), lambda i: (0, 0)),
            pl.BlockSpec((hidden, width), lambda i: (0, 0)),
        ],
        out_specs=pl.BlockSpec((tile, width), lambda i: (i, 0)),
        out_shape=jax.ShapeDtypeStruct((n_rows, width), dtype),
        cost_estimate=pl.CostEstimate(
            flops=6 * n_rows * width * hidden, bytes_accessed=14 << 20, transcendentals=0
        ),
        name="expert",
    )(rows, w_gate, w_up, w_down)


def combine_body(high_ref, low_ref, rows_ref, shared_ref, out_ref):
    rows = rows_ref[...]
    total = dot_tn(high_ref[...], rows) + dot_tn(low_ref[...], rows) + shared_ref[...]
    out_ref[...] = total.astype(BF16)


def combine(high, low, rows, shared):
    n_slots, n_tokens = high.shape
    width = rows.shape[1]
    tile = width // 4
    return pl.pallas_call(
        combine_body,
        grid=(width // tile,),
        in_specs=[
            pl.BlockSpec((n_slots, n_tokens), lambda i: (0, 0)),
            pl.BlockSpec((n_slots, n_tokens), lambda i: (0, 0)),
            pl.BlockSpec((n_slots, tile), lambda i: (0, i)),
            pl.BlockSpec((n_tokens, tile), lambda i: (0, i)),
        ],
        out_specs=pl.BlockSpec((n_tokens, tile), lambda i: (0, i)),
        out_shape=jax.ShapeDtypeStruct((n_tokens, width), BF16),
        cost_estimate=pl.CostEstimate(
            flops=4 * n_tokens * n_slots * width, bytes_accessed=6 << 20, transcendentals=0
        ),
        name="combine",
    )(high, low, rows, shared)


def exchange(x, axes):
    return lax.all_to_all(x, axes, split_axis=0, concat_axis=0, tiled=True)


def local(
    query_rows,
    key_rows,
    value_rows,
    gate_rows,
    log_decay,
    out_proj,
    moe_input,
    norm_gain,
    routing,
    route_weight,
    expert_gate,
    expert_up,
    expert_down,
    shared_gate,
    shared_up,
    shared_down,
):
    n_rows = query_rows.shape[0]
    width = moe_input.shape[1]
    tp = lax.axis_size("tp")
    experts = lax.axis_size(EP) * tp

    n_tokens = moe_input.shape[0]
    places = lax.axis_size(EP)
    routes, route_weights = routing.T, route_weight.T
    message = norm(moe_input, norm_gain, routes)
    messages = all_shifts(message, "tp")

    pieces = end_state(key_rows, value_rows, log_decay)
    pieces = exchange(pieces, EP)
    pieces = prefixes(pieces)
    incoming = exchange(pieces, EP).reshape(-1, DV)

    outgoing = dispatch(messages, experts * CAP)
    received = exchange(outgoing.reshape(places, tp * CAP, width), EP)

    own, other = gather_projection(out_proj)

    retained = mixer(query_rows, key_rows, value_rows, gate_rows, log_decay, incoming)
    retained = retained.reshape(tp, n_rows // tp, -1)
    place = lax.axis_index("tp")
    heads = []
    for d in range(1, tp):
        block = lax.dynamic_index_in_dim(retained, (place + d) % tp, keepdims=False)
        heads.append(shift(block, "tp", d))

    shared = expert_apply(message, shared_gate, shared_up, shared_down, F32, n_tokens)
    high, low = slot_weights(routes, route_weights, experts * CAP)

    served = expert_apply(
        received.reshape(-1, width), expert_gate[0], expert_up[0], expert_down[0], BF16
    )
    returned = exchange(served.reshape(experts, CAP, width), EP_TP)

    mixer_out = project(retained, heads, out_proj, own, other)
    moe_out = combine(high, low, returned.reshape(-1, width), shared)
    return (mixer_out, moe_out)


def solution(mesh):
    split = Mesh(mesh.devices.reshape(4, 4, 2, mesh.shape["tp"]), ("ep_0", "ep_1", "ep_2", "tp"))
    return jax.shard_map(
        local,
        mesh=split,
        in_specs=(
            P(EP, "tp"),
            P(EP, "tp"),
            P(EP, "tp"),
            P(EP, "tp"),
            P("tp", EP),
            P("tp", None),
            P(EP_TP, None),
            P(),
            P(EP_TP, None),
            P(EP_TP, None),
            P(EP_TP, None, None),
            P(EP_TP, None, None),
            P(EP_TP, None, None),
            P(),
            P(),
            P(),
        ),
        out_specs=(P(EP_TP, None), P(EP_TP, None)),
        check_vma=False,
    )
```

```python
import functools

import jax
import jax.numpy as jnp
from jax import lax
from jax.experimental import pallas as pl
from jax.experimental.pallas import tpu as pltpu
from jax.sharding import Mesh
from jax.sharding import PartitionSpec as P


DK = 128
DV = 256
BLOCK = 128
CAP = 8
NOTE = 16
EP = ("ep_0", "ep_1", "ep_2")
EP_TP = ("ep_0", "ep_1", "ep_2", "tp")
EPS = 1e-06
ALL_VMEM = pltpu.CompilerParams(vmem_limit_bytes=67043328)
SCALE = DK ** (-0.5)
F32 = jnp.float32
BF16 = jnp.bfloat16


def iota(shape, dim):
    return lax.broadcasted_iota(jnp.int32, shape, dim)


def dot(a, b):
    return jnp.dot(a, b, preferred_element_type=F32)


def dot_nt(a, b):
    return lax.dot_general(a, b, (((1,), (1,)), ((), ())), preferred_element_type=F32)


def dot_tn(a, b):
    return lax.dot_general(a, b, (((0,), (0,)), ((), ())), preferred_element_type=F32)


def silu(v):
    return v / (1.0 + jnp.exp(-v))


def thirds(a):
    high = a.astype(BF16)
    rest = a - high.astype(F32)
    middle = rest.astype(BF16)
    return high, middle, (rest - middle.astype(F32)).astype(BF16)


def sums_down(pick, a):
    return sum(dot_nt(pick, part) for part in thirds(a))


def sums_across(a, pick):
    return sum(dot(part, pick) for part in thirds(a))


def write_message(ref, h, state, total):
    whole = jnp.broadcast_to(total, (NOTE, DV))
    high = whole.astype(BF16).astype(F32)
    middle = (whole - high).astype(BF16).astype(F32)
    row = iota((NOTE, DV), 0)
    note = jnp.where(row == 0, high, jnp.where(row == 1, middle, whole - high - middle))
    ref[h, :DK] = state.astype(BF16)
    ref[h, DK:] = note.astype(BF16)


def read_message(ref, k, h):
    note = ref[k, h, DK:].astype(F32)
    return ref[k, h, :DK].astype(F32), note[0:1] + note[1:2] + note[2:3]


def end_state_body(k_ref, v_ref, a_ref, out_ref, state, total):
    step = pl.program_id(0)

    @pl.when(step == 0)
    def _():
        state[...] = jnp.zeros_like(state)
        total[...] = jnp.zeros_like(total)

    n_heads = a_ref.shape[0]
    n_blocks = k_ref.shape[0] // BLOCK
    after = iota((BLOCK, BLOCK), 1) > iota((BLOCK, BLOCK), 0)
    pick = jnp.where(after, 1.0, 0.0).astype(BF16)
    later = jnp.zeros((n_heads, 1), F32)
    keys = [[] for _ in range(n_heads)]
    for b in reversed(range(n_blocks)):
        rows = pl.ds(b * BLOCK, BLOCK)
        a = a_ref[:, rows]
        left = sums_down(pick, a)
        for h in range(n_heads):
            k = k_ref[rows, h * DK : (h + 1) * DK].astype(F32)
            fade = SCALE * jnp.exp(left[:, h : h + 1] + later[h : h + 1, :])
            keys[h].insert(0, (k * fade).astype(BF16))
        later = later + jnp.sum(a, axis=1, keepdims=True)
    for h in range(n_heads):
        gone = later[h : h + 1, :]
        added = dot_tn(jnp.concatenate(keys[h], axis=0), v_ref[:, h * DV : (h + 1) * DV])
        state[h] = state[h] * jnp.exp(gone) + added
        total[h] = total[h] + gone

    @pl.when(step == pl.num_programs(0) - 1)
    def _():
        for h in range(n_heads):
            write_message(out_ref, h, state[h], total[h, 0:1, 0:1])


def end_state(key_rows, value_rows, log_decay):
    n_rows, n_heads = key_rows.shape[0], log_decay.shape[0]
    tile = min(512, n_rows)
    return pl.pallas_call(
        end_state_body,
        grid=(n_rows // tile,),
        in_specs=[
            pl.BlockSpec((tile, n_heads * DK), lambda i: (i, 0)),
            pl.BlockSpec((tile, n_heads * DV), lambda i: (i, 0)),
            pl.BlockSpec((n_heads, tile), lambda i: (0, i)),
        ],
        out_specs=pl.BlockSpec((n_heads, DK + NOTE, DV), lambda i: (0, 0, 0)),
        out_shape=jax.ShapeDtypeStruct((n_heads, DK + NOTE, DV), BF16),
        scratch_shapes=[
            pltpu.VMEM((n_heads, DK, DV), F32),
            pltpu.VMEM((n_heads, 8, 128), F32),
        ],
        cost_estimate=pl.CostEstimate(
            flops=2 * n_rows * n_heads * DK * DV, bytes_accessed=4 << 20, transcendentals=0
        ),
        compiler_params=ALL_VMEM,
        name="end_state",
    )(key_rows, value_rows, log_decay)


def join_body(axis, peers, first, last, *refs):
    messages, refs = refs[:peers], refs[peers:]
    if not first:
        before_ref, refs = refs[0], refs[1:]
    ordered = refs[-1]
    me = lax.axis_index(axis)
    for d in range(peers):
        ordered[(me - d + peers) % peers] = messages[d][...]
    for h in range(refs[0].shape[0]):
        running, ahead = jnp.zeros((DK, DV), F32), jnp.zeros((DK, DV), F32)
        total, ahead_total = jnp.zeros((1, DV), F32), jnp.zeros((1, DV), F32)
        for k in range(peers):
            ahead = jnp.where(k == me, running, ahead)
            ahead_total = jnp.where(k == me, total, ahead_total)
            if last and k == peers - 1:
                break
            state, gone = read_message(ordered, k, h)
            running = running * jnp.exp(gone) + state
            total = total + gone
        if not first:
            gone = before_ref[h, DK : DK + 1]
            ahead = ahead * jnp.exp(gone) + before_ref[h, :DK]
            ahead_total = ahead_total + gone
        refs[0][h, :DK] = ahead
        refs[0][h, DK:] = jnp.broadcast_to(ahead_total, (8, DV))
        if not last:
            write_message(refs[1], h, running, total)


def join(axis, messages, before, last):
    peers = len(messages)
    n_heads = messages[0].shape[0]
    out = [jax.ShapeDtypeStruct((n_heads, DK + 8, DV), F32)]
    if not last:
        out.append(jax.ShapeDtypeStruct(messages[0].shape, BF16))
    return pl.pallas_call(
        functools.partial(join_body, axis, peers, before is None, last),
        out_shape=out,
        scratch_shapes=[pltpu.VMEM((peers,) + messages[0].shape, BF16)],
        cost_estimate=pl.CostEstimate(flops=1 << 22, bytes_accessed=2 << 20, transcendentals=0),
        compiler_params=ALL_VMEM,
        name="join",
    )(*messages, *([] if before is None else [before]))


def shift(x, axis, d):
    peers = lax.axis_size(axis)
    return lax.ppermute(x, axis, [(k, (k + d) % peers) for k in range(peers)])


def all_shifts(x, axis):
    return [x] + [shift(x, axis, d) for d in range(1, lax.axis_size(axis))]


def mixer_body(q_ref, k_ref, v_ref, g_ref, a_ref, first_ref, out_ref, state):
    @pl.when(pl.program_id(0) == 0)
    def _():
        state[...] = first_ref[:, :DK]

    n_heads = a_ref.shape[0]
    t, m = iota((BLOCK, BLOCK), 0), iota((BLOCK, BLOCK), 1)
    causal = t >= m
    upto = jnp.where(t <= m, 1.0, 0.0).astype(BF16)
    downto = jnp.where(causal, 1.0, 0.0).astype(BF16)
    for b in range(q_ref.shape[0] // BLOCK):
        rows = pl.ds(b * BLOCK, BLOCK)
        a = a_ref[:, rows]
        down = sums_down(downto, a)
        across = sums_across(a, upto)
        for h in range(n_heads):
            q = q_ref[rows, h * DK : (h + 1) * DK]
            k = k_ref[rows, h * DK : (h + 1) * DK]
            v = v_ref[rows, h * DV : (h + 1) * DV]
            gate = g_ref[rows, h * DV : (h + 1) * DV].astype(F32)
            col, row = down[:, h : h + 1], across[h : h + 1, :]
            whole = row[:, BLOCK - 1 : BLOCK]
            decay = jnp.where(causal, jnp.exp(jnp.where(causal, col - row, 0.0)), 0.0)
            weight = (dot_nt(q, k) * SCALE * decay).astype(BF16)
            before = state[h]
            raw = dot(weight, v) + dot(q, before.astype(BF16)) * jnp.exp(col)
            faded = (k.astype(F32) * (SCALE * jnp.exp(whole - col))).astype(BF16)
            state[h] = before * jnp.exp(whole) + dot_tn(faded, v)
            centered = raw - jnp.mean(raw, axis=1, keepdims=True)
            spread = jnp.mean(centered * centered, axis=1, keepdims=True)
            normed = centered * lax.rsqrt(spread + EPS)
            out_ref[rows, h * DV : (h + 1) * DV] = (silu(gate) * normed).astype(BF16)


def mixer(query_rows, key_rows, value_rows, gate_rows, log_decay, incoming):
    n_rows, n_heads = query_rows.shape[0], log_decay.shape[0]
    tile = min(256, n_rows)
    return pl.pallas_call(
        mixer_body,
        grid=(n_rows // tile,),
        in_specs=[
            pl.BlockSpec((tile, n_heads * DK), lambda i: (i, 0)),
            pl.BlockSpec((tile, n_heads * DK), lambda i: (i, 0)),
            pl.BlockSpec((tile, n_heads * DV), lambda i: (i, 0)),
            pl.BlockSpec((tile, n_heads * DV), lambda i: (i, 0)),
            pl.BlockSpec((n_heads, tile), lambda i: (0, i)),
            pl.BlockSpec((n_heads, DK + 8, DV), lambda i: (0, 0, 0)),
        ],
        out_specs=pl.BlockSpec((tile, n_heads * DV), lambda i: (i, 0)),
        out_shape=jax.ShapeDtypeStruct((n_rows, n_heads * DV), BF16),
        scratch_shapes=[pltpu.VMEM((n_heads, DK, DV), F32)],
        cost_estimate=pl.CostEstimate(
            flops=12 * n_rows * n_heads * DK * DV, bytes_accessed=8 << 20, transcendentals=0
        ),
        compiler_params=ALL_VMEM,
        name="mixer",
    )(query_rows, key_rows, value_rows, gate_rows, log_decay, incoming)


def project_body(*refs):
    heads, whole, own, other, out_ref, lhs, rhs, sems = (
        refs[:4],
        refs[4],
        refs[5:9],
        refs[9:13],
        *refs[13:],
    )
    x, core = lax.axis_index("tp"), lax.axis_index("ep_2")
    half = rhs.shape[-1]
    pairs = [(heads[0].at[x], lhs.at[0])]
    for d in range(1, 4):
        pairs.append((heads[d], lhs.at[d]))
    for side in range(2):
        pairs.append((whole.at[:, side * half : (side + 1) * half], rhs.at[0, side]))
    cut = rhs.shape[2] // 2
    for parts, side in ((own, core), (other, 1 - core)):
        pairs.append((parts[0], rhs.at[1, side]))
        pairs.append((parts[1], rhs.at[2, side, :cut]))
        pairs.append((parts[2], rhs.at[2, side, cut:]))
        pairs.append((parts[3], rhs.at[3, side]))
    copies = [
        pltpu.make_async_copy(source, target, sems.at[n])
        for n, (source, target) in enumerate(pairs)
    ]
    for copy in copies:
        copy.start()
    for copy in copies:
        copy.wait()
    fine = half // 2
    for side in range(2):
        for part in range(2):
            at = slice(part * fine, (part + 1) * fine)
            total = dot(lhs[0], rhs[0, side, :, at])
            for d in range(1, 4):
                total = total + dot(lhs[d], rhs[d, side, :, at])
            start = side * half + part * fine
            out_ref[:, start : start + fine] = total.astype(BF16)


def project(retained, received, whole, own, other):
    groups, n_rows, width = retained.shape
    half = whole.shape[1] // 2
    arrays = [retained, *received, whole, *own, *other]
    return pl.pallas_call(
        project_body,
        in_specs=[pl.BlockSpec(memory_space=pl.ANY)] * len(arrays),
        out_shape=jax.ShapeDtypeStruct((n_rows, 2 * half), BF16),
        scratch_shapes=[
            pltpu.VMEM((groups, n_rows, width), BF16),
            pltpu.VMEM((groups, 2, width, half), BF16),
            pltpu.SemaphoreType.DMA((14,)),
        ],
        cost_estimate=pl.CostEstimate(
            flops=4 * n_rows * groups * width * half, bytes_accessed=12 << 20, transcendentals=0
        ),
        compiler_params=ALL_VMEM,
        name="project",
    )(*arrays)


def gather_projection(out_proj):
    n_rows, width = out_proj.shape
    half, cut = width // 2, n_rows // 2
    mine = lax.dynamic_slice(out_proj, (0, lax.axis_index("ep_2") * half), (n_rows, half))
    below, above = shift(mine, "tp", 1), shift(mine, "tp", 3)
    far = [shift(below[:cut], "tp", 1), shift(above[cut:], "tp", 3)]
    own = [below, *far, above]
    other = [shift(part, "ep_2", 1) for part in own]
    return own, other


def norm_body(x_ref, gain_ref, route_ref, out_ref):
    x = x_ref[...].astype(F32)
    n_tokens = x.shape[0]
    mean = jnp.mean(x * x, axis=1, keepdims=True)
    out_ref[:n_tokens] = (x * lax.rsqrt(mean + EPS) * gain_ref[...]).astype(BF16)
    row = iota((NOTE, n_tokens), 0)
    note = jnp.zeros((NOTE, n_tokens), F32)
    for k in range(route_ref.shape[0]):
        note = jnp.where(row == k, route_ref[k : k + 1].astype(F32), note)
    out_ref[n_tokens:, :n_tokens] = note.astype(BF16)
    rest = (NOTE, x.shape[1] - n_tokens)
    out_ref[n_tokens:, n_tokens:] = jnp.zeros(rest, BF16)


def norm(moe_input, norm_gain, routes):
    n_tokens, width = moe_input.shape
    return pl.pallas_call(
        norm_body,
        out_shape=jax.ShapeDtypeStruct((n_tokens + NOTE, width), BF16),
        compiler_params=ALL_VMEM,
        name="norm",
    )(moe_input, norm_gain.reshape(1, width), routes)


def ranked(hits, n_tokens, none=float(CAP)):
    earlier = iota((n_tokens, n_tokens), 0) < iota((n_tokens, n_tokens), 1)
    rank = dot(hits.astype(BF16), jnp.where(earlier, 1.0, 0.0).astype(BF16))
    return jnp.where(hits > 0.0, rank, none).astype(BF16)


def dispatch_body(*refs):
    messages, out_ref, picks = refs[:-2], refs[-2], refs[-1]
    groups = len(messages)
    n_slots = out_ref.shape[0]
    each = groups * CAP
    experts = n_slots // each
    n_tokens = messages[0].shape[0] - NOTE

    @pl.when(pl.program_id(0) == 0)
    def _():
        x = lax.axis_index("tp")
        expert = (iota((experts, n_tokens), 0) * groups + x).astype(F32)
        shape = (n_slots, experts)
        low = iota(shape, 1) * each
        row = iota(shape, 0)
        owner = jnp.where((row >= low) & (row < low + each), 1.0, 0.0).astype(BF16)
        slot = iota((n_slots, n_tokens), 0)
        spot = slot & (each - 1)
        for d in range(groups):
            named = messages[d][n_tokens:, :n_tokens].astype(F32)
            hits = jnp.zeros((experts, n_tokens), F32)
            for k in range(4):
                hits = jnp.where(named[k : k + 1] == expert, 1.0, hits)
            start = ((x - d + groups) % groups) * CAP
            rank = dot(owner, ranked(hits, n_tokens, 64.0))
            pick = jnp.where(rank == (spot - start).astype(F32), 1.0, 0.0).astype(BF16)
            picks[:, d * n_tokens : (d + 1) * n_tokens] = pick

    rows = jnp.concatenate([message[:n_tokens] for message in messages], axis=0)
    out_ref[...] = dot(picks[...], rows).astype(BF16)


def dispatch(messages, n_slots):
    n_rows, width = messages[0].shape
    groups, tile = len(messages), width // 4
    return pl.pallas_call(
        dispatch_body,
        grid=(width // tile,),
        in_specs=[pl.BlockSpec((n_rows, tile), lambda i: (0, i))] * groups,
        out_specs=pl.BlockSpec((n_slots, tile), lambda i: (0, i)),
        out_shape=jax.ShapeDtypeStruct((n_slots, width), BF16),
        scratch_shapes=[pltpu.VMEM((n_slots, groups * (n_rows - NOTE)), BF16)],
        compiler_params=ALL_VMEM,
        cost_estimate=pl.CostEstimate(
            flops=1024 * n_slots * width, bytes_accessed=6 << 20, transcendentals=0
        ),
        name="dispatch",
    )(*messages)


def weights_body(route_ref, weight_ref, out_ref):
    n_visits, n_tokens = route_ref.shape
    n_slots = out_ref.shape[1]
    experts = n_slots // CAP
    expert = iota((experts, n_tokens), 0)
    hits = jnp.zeros((experts, n_tokens), F32)
    weighed = jnp.zeros((experts, n_tokens), F32)
    for k in range(n_visits):
        hit = route_ref[k : k + 1] == expert
        hits = jnp.where(hit, 1.0, hits)
        weighed = jnp.where(hit, weight_ref[k : k + 1], weighed)
    spread = jnp.where(iota((n_slots, experts), 0) // CAP == iota((n_slots, experts), 1), 1.0, 0.0)
    spread = spread.astype(BF16)
    place = (iota((n_slots, n_tokens), 0) % CAP).astype(F32)
    here = dot(spread, ranked(hits, n_tokens)) == place
    high = weighed.astype(BF16)
    low = (weighed - high.astype(F32)).astype(BF16)
    out_ref[:n_tokens] = jnp.where(here, dot(spread, high), 0.0).T.astype(BF16)
    out_ref[n_tokens:] = jnp.where(here, dot(spread, low), 0.0).T.astype(BF16)


def slot_weights(routes, route_weights, n_slots):
    n_tokens = routes.shape[1]
    return pl.pallas_call(
        weights_body,
        out_shape=jax.ShapeDtypeStruct((2 * n_tokens, n_slots), BF16),
        compiler_params=ALL_VMEM,
        cost_estimate=pl.CostEstimate(flops=1 << 27, bytes_accessed=1 << 20, transcendentals=0),
        name="weights",
    )(routes, route_weights)


def expert_body(x_ref, gate_ref, up_ref, down_ref, out_ref):
    x = x_ref[...]
    hidden = (silu(dot(x, gate_ref[...])) * dot(x, up_ref[...])).astype(BF16)
    out_ref[...] = dot(hidden, down_ref[...]).astype(out_ref.dtype)


def expert_apply(rows, w_gate, w_up, w_down, dtype, n_rows=None):
    n_rows, width = n_rows or rows.shape[0], rows.shape[1]
    hidden = w_gate.shape[1]
    tile = min(512, n_rows)
    return pl.pallas_call(
        expert_body,
        grid=(n_rows // tile,),
        in_specs=[
            pl.BlockSpec((tile, width), lambda i: (i, 0)),
            pl.BlockSpec((width, hidden), lambda i: (0, 0)),
            pl.BlockSpec((width, hidden), lambda i: (0, 0)),
            pl.BlockSpec((hidden, width), lambda i: (0, 0)),
        ],
        out_specs=pl.BlockSpec((tile, width), lambda i: (i, 0)),
        out_shape=jax.ShapeDtypeStruct((n_rows, width), dtype),
        cost_estimate=pl.CostEstimate(
            flops=6 * n_rows * width * hidden, bytes_accessed=14 << 20, transcendentals=0
        ),
        compiler_params=ALL_VMEM,
        name="expert",
    )(rows, w_gate, w_up, w_down)


def combine_body(weight_ref, rows_ref, shared_ref, out_ref):
    both = dot(weight_ref[...], rows_ref[...])
    n_tokens = out_ref.shape[0]
    out_ref[...] = (both[:n_tokens] + both[n_tokens:] + shared_ref[...]).astype(BF16)


def combine(weights, rows, shared):
    n_slots, width = rows.shape
    n_tokens = shared.shape[0]
    tile = width // 4
    return pl.pallas_call(
        combine_body,
        grid=(width // tile,),
        in_specs=[
            pl.BlockSpec((2 * n_tokens, n_slots), lambda i: (0, 0)),
            pl.BlockSpec((n_slots, tile), lambda i: (0, i)),
            pl.BlockSpec((n_tokens, tile), lambda i: (0, i)),
        ],
        out_specs=pl.BlockSpec((n_tokens, tile), lambda i: (0, i)),
        out_shape=jax.ShapeDtypeStruct((n_tokens, width), BF16),
        cost_estimate=pl.CostEstimate(
            flops=4 * n_tokens * n_slots * width, bytes_accessed=6 << 20, transcendentals=0
        ),
        compiler_params=ALL_VMEM,
        name="combine",
    )(weights, rows, shared)


def exchange(x, axes):
    return lax.all_to_all(x, axes, split_axis=0, concat_axis=0, tiled=True)


def local(
    query_rows,
    key_rows,
    value_rows,
    gate_rows,
    log_decay,
    out_proj,
    moe_input,
    norm_gain,
    routing,
    route_weight,
    expert_gate,
    expert_up,
    expert_down,
    shared_gate,
    shared_up,
    shared_down,
):
    n_rows = query_rows.shape[0]
    width = moe_input.shape[1]
    tp = lax.axis_size("tp")
    experts = lax.axis_size(EP) * tp

    n_tokens = moe_input.shape[0]
    places = lax.axis_size(EP)
    routes, route_weights = routing.T, route_weight.T
    message = norm(moe_input, norm_gain, routes)
    messages = all_shifts(message, "tp")

    state = end_state(key_rows, value_rows, log_decay)
    before = None
    for axis in reversed(EP):
        travelled = all_shifts(state, axis)
        before, *state = join(axis, travelled, before, axis == EP[0])
        state = state[0] if state else None

    outgoing = dispatch(messages, experts * CAP)
    received = exchange(outgoing.reshape(places, tp * CAP, width), EP)

    own, other = gather_projection(out_proj)

    retained = mixer(query_rows, key_rows, value_rows, gate_rows, log_decay, before)
    retained = retained.reshape(tp, n_rows // tp, -1)
    place = lax.axis_index("tp")
    heads = []
    for d in range(1, tp):
        block = lax.dynamic_index_in_dim(retained, (place + d) % tp, keepdims=False)
        heads.append(shift(block, "tp", d))

    shared = expert_apply(message, shared_gate, shared_up, shared_down, F32, n_tokens)
    weights = slot_weights(routes, route_weights, experts * CAP)

    served = expert_apply(
        received.reshape(-1, width), expert_gate[0], expert_up[0], expert_down[0], BF16
    )
    returned = exchange(served.reshape(experts, CAP, width), EP_TP)

    mixer_out = project(retained, heads, out_proj, own, other)
    moe_out = combine(weights, returned.reshape(-1, width), shared)
    return (mixer_out, moe_out)


def solution(mesh):
    split = Mesh(mesh.devices.reshape(4, 4, 2, mesh.shape["tp"]), ("ep_0", "ep_1", "ep_2", "tp"))
    return jax.shard_map(
        local,
        mesh=split,
        in_specs=(
            P(EP, "tp"),
            P(EP, "tp"),
            P(EP, "tp"),
            P(EP, "tp"),
            P("tp", EP),
            P("tp", None),
            P(EP_TP, None),
            P(),
            P(EP_TP, None),
            P(EP_TP, None),
            P(EP_TP, None, None),
            P(EP_TP, None, None),
            P(EP_TP, None, None),
            P(),
            P(),
            P(),
        ),
        out_specs=(P(EP_TP, None), P(EP_TP, None)),
        check_vma=False,
    )
```

```python
import functools

import jax
import jax.numpy as jnp
from jax import lax
from jax.experimental import pallas as pl
from jax.experimental.pallas import tpu as pltpu
from jax.sharding import Mesh
from jax.sharding import PartitionSpec as P


DK = 128
DV = 256
BLOCK = 128
CAP = 8
NOTE = 16
ROUTE = 8
EP = ("ep_0", "ep_1", "ep_2")
EP_TP = ("ep_0", "ep_1", "ep_2", "tp")
EPS = 1e-06
ALL_VMEM = pltpu.CompilerParams(vmem_limit_bytes=67043328)
SCALE = DK ** (-0.5)
F32 = jnp.float32
BF16 = jnp.bfloat16


def iota(shape, dim):
    return lax.broadcasted_iota(jnp.int32, shape, dim)


def dot(a, b):
    return jnp.dot(a, b, preferred_element_type=F32)


def dot_nt(a, b):
    return lax.dot_general(a, b, (((1,), (1,)), ((), ())), preferred_element_type=F32)


def dot_tn(a, b):
    return lax.dot_general(a, b, (((0,), (0,)), ((), ())), preferred_element_type=F32)


def silu(v):
    return v / (1.0 + jnp.exp(-v))


def thirds(a):
    high = a.astype(BF16)
    rest = a - high.astype(F32)
    middle = rest.astype(BF16)
    return high, middle, (rest - middle.astype(F32)).astype(BF16)


def sums_down(pick, a):
    return sum(dot_nt(pick, part) for part in thirds(a))


def sums_across(a, pick):
    return sum(dot(part, pick) for part in thirds(a))


def write_message(ref, state, total):
    whole = jnp.broadcast_to(total, (NOTE, DV))
    high, middle, low = (part.astype(F32) for part in thirds(whole))
    row = iota((NOTE, DV), 0)
    ref[:DK] = state.astype(BF16)
    ref[DK:] = jnp.where(row == 0, high, jnp.where(row == 1, middle, low)).astype(BF16)


def read_message(ref):
    note = ref[DK:].astype(F32)
    return ref[:DK].astype(F32), note[0:1] + note[1:2] + note[2:3]


def end_state_body(k_ref, v_ref, a_ref, keep_ref, give_ref, state, total):
    step = pl.program_id(0)

    @pl.when(step == 0)
    def _():
        state[...] = jnp.zeros_like(state)
        total[...] = jnp.zeros_like(total)

    n_heads = a_ref.shape[0]
    n_blocks = k_ref.shape[0] // BLOCK
    after = iota((BLOCK, BLOCK), 1) > iota((BLOCK, BLOCK), 0)
    pick = jnp.where(after, 1.0, 0.0).astype(BF16)
    later = jnp.zeros((n_heads, 1), F32)
    keys = [[] for _ in range(n_heads)]
    for b in reversed(range(n_blocks)):
        rows = pl.ds(b * BLOCK, BLOCK)
        a = a_ref[:, rows]
        left = sums_down(pick, a)
        for h in range(n_heads):
            k = k_ref[rows, h * DK : (h + 1) * DK].astype(F32)
            fade = SCALE * jnp.exp(left[:, h : h + 1] + later[h : h + 1, :])
            keys[h].insert(0, (k * fade).astype(BF16))
        later = later + jnp.sum(a, axis=1, keepdims=True)
    for h in range(n_heads):
        gone = later[h : h + 1, :]
        added = dot_tn(jnp.concatenate(keys[h], axis=0), v_ref[:, h * DV : (h + 1) * DV])
        state[h] = state[h] * jnp.exp(gone) + added
        total[h] = total[h] + gone

    @pl.when(step == pl.num_programs(0) - 1)
    def _():
        core = lax.axis_index("ep_2")
        write_message(keep_ref, state[core], total[core][0:1, 0:1])
        write_message(give_ref, state[1 - core], total[1 - core][0:1, 0:1])


def end_state(key_rows, value_rows, log_decay):
    n_rows, n_heads = key_rows.shape[0], log_decay.shape[0]
    tile = min(512, n_rows)
    return pl.pallas_call(
        end_state_body,
        grid=(n_rows // tile,),
        in_specs=[
            pl.BlockSpec((tile, n_heads * DK), lambda i: (i, 0)),
            pl.BlockSpec((tile, n_heads * DV), lambda i: (i, 0)),
            pl.BlockSpec((n_heads, tile), lambda i: (0, i)),
        ],
        out_specs=[pl.BlockSpec((DK + NOTE, DV), lambda i: (0, 0))] * 2,
        out_shape=[jax.ShapeDtypeStruct((DK + NOTE, DV), BF16)] * 2,
        scratch_shapes=[
            pltpu.VMEM((n_heads, DK, DV), F32),
            pltpu.VMEM((n_heads, 8, 128), F32),
        ],
        cost_estimate=pl.CostEstimate(
            flops=2 * n_rows * n_heads * DK * DV, bytes_accessed=4 << 20, transcendentals=0
        ),
        compiler_params=ALL_VMEM,
        name="end_state",
    )(key_rows, value_rows, log_decay)


def join_cores_body(keep_ref, got_ref, out_ref):
    core = lax.axis_index("ep_2")
    keep, kept = read_message(keep_ref)
    got, gone = read_message(got_ref)
    first = core == 0
    joined = jnp.where(first, keep * jnp.exp(gone) + got, got * jnp.exp(kept) + keep)
    write_message(out_ref, joined, kept + gone)


def join_cores(keep, got):
    return pl.pallas_call(
        join_cores_body,
        out_shape=jax.ShapeDtypeStruct(keep.shape, BF16),
        compiler_params=ALL_VMEM,
        name="join_cores",
    )(keep, got)


def join(axis, messages, ordered):
    peers, me = len(messages), lax.axis_index(axis)
    for d in range(peers):
        ordered[(me - d + peers) % peers] = messages[d][...]
    running, ahead = jnp.zeros((DK, DV), F32), jnp.zeros((DK, DV), F32)
    total, ahead_total = jnp.zeros((1, DV), F32), jnp.zeros((1, DV), F32)
    for k in range(peers):
        ahead = jnp.where(k == me, running, ahead)
        ahead_total = jnp.where(k == me, total, ahead_total)
        state, gone = read_message(ordered.at[k])
        running = running * jnp.exp(gone) + state
        total = total + gone
    return ahead, ahead_total, running, total


def join_plane_body(*refs):
    messages, (before_ref, all_ref, ordered) = refs[:-3], refs[-3:]
    ahead, gone, running, total = join("ep_1", messages, ordered)
    before_ref[:DK] = ahead
    before_ref[DK:] = jnp.broadcast_to(gone, (8, DV))
    write_message(all_ref, running, total)


def join_plane(messages):
    shape = messages[0].shape
    return pl.pallas_call(
        join_plane_body,
        out_shape=[
            jax.ShapeDtypeStruct((DK + 8, DV), F32),
            jax.ShapeDtypeStruct(shape, BF16),
        ],
        scratch_shapes=[pltpu.VMEM((len(messages),) + shape, BF16)],
        compiler_params=ALL_VMEM,
        cost_estimate=pl.CostEstimate(flops=1 << 22, bytes_accessed=1 << 20, transcendentals=0),
        name="join_plane",
    )(*messages)


def join_last_body(*refs):
    messages, (before_ref, keep_ref, got_ref, mine_ref, theirs_ref, ordered) = refs[:-6], refs[-6:]
    ahead, _, _, _ = join("ep_0", messages, ordered)
    gone = before_ref[DK : DK + 1]
    first = ahead * jnp.exp(gone) + before_ref[:DK]
    keep, kept = read_message(keep_ref)
    got, gone = read_message(got_ref)
    low = lax.axis_index("ep_2") == 0
    second = first * jnp.exp(jnp.where(low, kept, gone)) + jnp.where(low, keep, got)
    mine_ref[...] = jnp.where(low, first, second)
    theirs_ref[...] = jnp.where(low, second, first).astype(BF16)


def join_last(messages, before, keep, got):
    shape = messages[0].shape
    return pl.pallas_call(
        join_last_body,
        out_shape=[
            jax.ShapeDtypeStruct((DK, DV), F32),
            jax.ShapeDtypeStruct((DK, DV), BF16),
        ],
        scratch_shapes=[pltpu.VMEM((len(messages),) + shape, BF16)],
        compiler_params=ALL_VMEM,
        cost_estimate=pl.CostEstimate(flops=1 << 22, bytes_accessed=1 << 20, transcendentals=0),
        name="join_last",
    )(*messages, before, keep, got)


def shift(x, axis, d):
    peers = lax.axis_size(axis)
    return lax.ppermute(x, axis, [(k, (k + d) % peers) for k in range(peers)])


def all_shifts(x, axis):
    return [x] + [shift(x, axis, d) for d in range(1, lax.axis_size(axis))]


def mixer_body(q_ref, k_ref, v_ref, g_ref, a_ref, mine_ref, theirs_ref, out_ref, state):
    @pl.when(pl.program_id(0) == 0)
    def _():
        core = lax.axis_index("ep_2")
        state[core] = mine_ref[...]
        state[1 - core] = theirs_ref[...].astype(F32)

    n_heads = a_ref.shape[0]
    t, m = iota((BLOCK, BLOCK), 0), iota((BLOCK, BLOCK), 1)
    causal = t >= m
    upto = jnp.where(t <= m, 1.0, 0.0).astype(BF16)
    downto = jnp.where(causal, 1.0, 0.0).astype(BF16)
    for b in range(q_ref.shape[0] // BLOCK):
        rows = pl.ds(b * BLOCK, BLOCK)
        a = a_ref[:, rows]
        down = sums_down(downto, a)
        across = sums_across(a, upto)
        for h in range(n_heads):
            q = q_ref[rows, h * DK : (h + 1) * DK]
            k = k_ref[rows, h * DK : (h + 1) * DK]
            v = v_ref[rows, h * DV : (h + 1) * DV]
            gate = g_ref[rows, h * DV : (h + 1) * DV].astype(F32)
            col, row = down[:, h : h + 1], across[h : h + 1, :]
            whole = row[:, BLOCK - 1 : BLOCK]
            decay = jnp.where(causal, jnp.exp(jnp.where(causal, col - row, 0.0)), 0.0)
            weight = (dot_nt(q, k) * SCALE * decay).astype(BF16)
            before = state[h]
            raw = dot(weight, v) + dot(q, before.astype(BF16)) * jnp.exp(col)
            faded = (k.astype(F32) * (SCALE * jnp.exp(whole - col))).astype(BF16)
            state[h] = before * jnp.exp(whole) + dot_tn(faded, v)
            centered = raw - jnp.mean(raw, axis=1, keepdims=True)
            spread = jnp.mean(centered * centered, axis=1, keepdims=True)
            normed = centered * lax.rsqrt(spread + EPS)
            out_ref[rows, h * DV : (h + 1) * DV] = (silu(gate) * normed).astype(BF16)


def mixer(query_rows, key_rows, value_rows, gate_rows, log_decay, mine, theirs):
    n_rows, n_heads = query_rows.shape[0], log_decay.shape[0]
    tile = min(256, n_rows)
    return pl.pallas_call(
        mixer_body,
        grid=(n_rows // tile,),
        in_specs=[
            pl.BlockSpec((tile, n_heads * DK), lambda i: (i, 0)),
            pl.BlockSpec((tile, n_heads * DK), lambda i: (i, 0)),
            pl.BlockSpec((tile, n_heads * DV), lambda i: (i, 0)),
            pl.BlockSpec((tile, n_heads * DV), lambda i: (i, 0)),
            pl.BlockSpec((n_heads, tile), lambda i: (0, i)),
            pl.BlockSpec((DK, DV), lambda i: (0, 0)),
            pl.BlockSpec((DK, DV), lambda i: (0, 0)),
        ],
        out_specs=pl.BlockSpec((tile, n_heads * DV), lambda i: (i, 0)),
        out_shape=jax.ShapeDtypeStruct((n_rows, n_heads * DV), BF16),
        scratch_shapes=[pltpu.VMEM((n_heads, DK, DV), F32)],
        cost_estimate=pl.CostEstimate(
            flops=12 * n_rows * n_heads * DK * DV, bytes_accessed=8 << 20, transcendentals=0
        ),
        compiler_params=ALL_VMEM,
        name="mixer",
    )(query_rows, key_rows, value_rows, gate_rows, log_decay, mine, theirs)


def project_body(*refs):
    heads, whole, own, other, out_ref, lhs, rhs, sems = (
        refs[:4],
        refs[4],
        refs[5:9],
        refs[9:13],
        *refs[13:],
    )
    x, core = lax.axis_index("tp"), lax.axis_index("ep_2")
    half = rhs.shape[-1]
    pairs = [(heads[0].at[x], lhs.at[0])]
    for d in range(1, 4):
        pairs.append((heads[d], lhs.at[d]))
    for side in range(2):
        pairs.append((whole.at[:, side * half : (side + 1) * half], rhs.at[0, side]))
    cut = rhs.shape[2] // 2
    for parts, side in ((own, core), (other, 1 - core)):
        pairs.append((parts[0], rhs.at[1, side]))
        pairs.append((parts[1], rhs.at[2, side, :cut]))
        pairs.append((parts[2], rhs.at[2, side, cut:]))
        pairs.append((parts[3], rhs.at[3, side]))
    copies = [
        pltpu.make_async_copy(source, target, sems.at[n])
        for n, (source, target) in enumerate(pairs)
    ]
    for copy in copies:
        copy.start()
    for copy in copies:
        copy.wait()
    fine = half // 2
    for side in range(2):
        for part in range(2):
            at = slice(part * fine, (part + 1) * fine)
            total = dot(lhs[0], rhs[0, side, :, at])
            for d in range(1, 4):
                total = total + dot(lhs[d], rhs[d, side, :, at])
            start = side * half + part * fine
            out_ref[:, start : start + fine] = total.astype(BF16)


def project(retained, received, whole, own, other):
    groups, n_rows, width = retained.shape
    half = whole.shape[1] // 2
    arrays = [retained, *received, whole, *own, *other]
    return pl.pallas_call(
        project_body,
        in_specs=[pl.BlockSpec(memory_space=pl.ANY)] * len(arrays),
        out_shape=jax.ShapeDtypeStruct((n_rows, 2 * half), BF16),
        scratch_shapes=[
            pltpu.VMEM((groups, n_rows, width), BF16),
            pltpu.VMEM((groups, 2, width, half), BF16),
            pltpu.SemaphoreType.DMA((14,)),
        ],
        cost_estimate=pl.CostEstimate(
            flops=4 * n_rows * groups * width * half, bytes_accessed=12 << 20, transcendentals=0
        ),
        compiler_params=ALL_VMEM,
        name="project",
    )(*arrays)


def gather_projection(out_proj):
    n_rows, width = out_proj.shape
    half, cut = width // 2, n_rows // 2
    mine = lax.dynamic_slice(out_proj, (0, lax.axis_index("ep_2") * half), (n_rows, half))
    below, above = shift(mine, "tp", 1), shift(mine, "tp", 3)
    far = [shift(below[:cut], "tp", 1), shift(above[cut:], "tp", 3)]
    own = [below, *far, above]
    other = [shift(part, "ep_2", 1) for part in own]
    return own, other


def norm_body(x_ref, gain_ref, route_ref, out_ref):
    x = x_ref[...].astype(F32)
    n_tokens = x.shape[0]
    mean = jnp.mean(x * x, axis=1, keepdims=True)
    out_ref[:n_tokens] = (x * lax.rsqrt(mean + EPS) * gain_ref[...]).astype(BF16)
    row = iota((ROUTE, n_tokens), 0)
    note = jnp.zeros((ROUTE, n_tokens), F32)
    for k in range(route_ref.shape[0]):
        note = jnp.where(row == k, route_ref[k : k + 1].astype(F32), note)
    out_ref[n_tokens:, :n_tokens] = note.astype(BF16)
    rest = (ROUTE, x.shape[1] - n_tokens)
    out_ref[n_tokens:, n_tokens:] = jnp.zeros(rest, BF16)


def norm(moe_input, norm_gain, routes):
    n_tokens, width = moe_input.shape
    return pl.pallas_call(
        norm_body,
        out_shape=jax.ShapeDtypeStruct((n_tokens + ROUTE, width), BF16),
        compiler_params=ALL_VMEM,
        name="norm",
    )(moe_input, norm_gain.reshape(1, width), routes)


def ranked(hits, n_tokens, none=float(CAP)):
    earlier = iota((n_tokens, n_tokens), 0) < iota((n_tokens, n_tokens), 1)
    rank = dot(hits.astype(BF16), jnp.where(earlier, 1.0, 0.0).astype(BF16))
    return jnp.where(hits > 0.0, rank, none).astype(BF16)


def slot_owners(n_slots):
    shape = (n_slots, n_slots // CAP)
    return jnp.where(iota(shape, 0) // CAP == iota(shape, 1), 1.0, 0.0).astype(BF16)


def picks_of(note, n_slots):
    n_tokens = note.shape[1]
    experts = n_slots // CAP
    line = lax.axis_size("tp")
    expert = (iota((experts, n_tokens), 0) * line + lax.axis_index("tp")).astype(F32)
    hits = jnp.zeros((experts, n_tokens), F32)
    for k in range(4):
        hits = jnp.where(note[k : k + 1] == expert, 1.0, hits)
    place = (iota((n_slots, n_tokens), 0) & (CAP - 1)).astype(F32)
    here = dot(slot_owners(n_slots), ranked(hits, n_tokens)) == place
    return jnp.where(here, 1.0, 0.0).astype(BF16)


def dispatch_body(shifts, *refs):
    n = len(shifts)
    messages, (out_ref, held, made, sems) = refs[:n], refs[-4:]
    experts, line, _, width = out_ref.shape
    n_tokens = held.shape[1] - ROUTE
    me = lax.axis_index("tp")
    arrive, leave = [], []
    for i, d in enumerate(shifts):
        to = out_ref.at[:, (me - d + line) % line]
        arrive.append(pltpu.make_async_copy(messages[i], held.at[i], sems.at[0, i]))
        leave.append(pltpu.make_async_copy(made.at[i], to, sems.at[1, i]))
    for copy in arrive:
        copy.start()
    for i in range(n):
        arrive[i].wait()
        pick = picks_of(held[i, n_tokens:, :n_tokens].astype(F32), experts * CAP)
        rows = dot(pick, held[i, :n_tokens])
        made[i] = rows.reshape(experts, CAP, width).astype(BF16)
        leave[i].start()
    for copy in leave:
        copy.wait()


def dispatch(messages, shifts, experts, outgoing=None):
    n, (n_rows, width) = len(messages), messages[0].shape
    arrays = list(messages) + ([] if outgoing is None else [outgoing])
    shape = (experts, lax.axis_size("tp"), CAP, width)
    return pl.pallas_call(
        functools.partial(dispatch_body, shifts),
        in_specs=[pl.BlockSpec(memory_space=pl.ANY)] * len(arrays),
        out_specs=pl.BlockSpec(memory_space=pl.ANY),
        out_shape=jax.ShapeDtypeStruct(shape, BF16),
        scratch_shapes=[
            pltpu.VMEM((n, n_rows, width), BF16),
            pltpu.VMEM((n, experts, CAP, width), BF16),
            pltpu.SemaphoreType.DMA((2, n)),
        ],
        input_output_aliases={} if outgoing is None else {n: 0},
        compiler_params=ALL_VMEM,
        cost_estimate=pl.CostEstimate(
            flops=256 * n * experts * CAP * width, bytes_accessed=2 * n << 20, transcendentals=0
        ),
        name="dispatch",
    )(*arrays)


def weights_body(route_ref, weight_ref, out_ref):
    n_visits, n_tokens = route_ref.shape
    n_slots = out_ref.shape[1]
    experts = n_slots // CAP
    expert = iota((experts, n_tokens), 0)
    hits = jnp.zeros((experts, n_tokens), F32)
    weighed = jnp.zeros((experts, n_tokens), F32)
    for k in range(n_visits):
        hit = route_ref[k : k + 1] == expert
        hits = jnp.where(hit, 1.0, hits)
        weighed = jnp.where(hit, weight_ref[k : k + 1], weighed)
    spread = jnp.where(iota((n_slots, experts), 0) // CAP == iota((n_slots, experts), 1), 1.0, 0.0)
    spread = spread.astype(BF16)
    place = (iota((n_slots, n_tokens), 0) % CAP).astype(F32)
    here = dot(spread, ranked(hits, n_tokens)) == place
    high = weighed.astype(BF16)
    low = (weighed - high.astype(F32)).astype(BF16)
    out_ref[:n_tokens] = jnp.where(here, dot(spread, high), 0.0).T.astype(BF16)
    out_ref[n_tokens:] = jnp.where(here, dot(spread, low), 0.0).T.astype(BF16)


def slot_weights(routes, route_weights, n_slots):
    n_tokens = routes.shape[1]
    return pl.pallas_call(
        weights_body,
        out_shape=jax.ShapeDtypeStruct((2 * n_tokens, n_slots), BF16),
        compiler_params=ALL_VMEM,
        cost_estimate=pl.CostEstimate(flops=1 << 27, bytes_accessed=1 << 20, transcendentals=0),
        name="weights",
    )(routes, route_weights)


def expert_body(x_ref, gate_ref, up_ref, down_ref, out_ref):
    x = x_ref[...]
    hidden = (silu(dot(x, gate_ref[...])) * dot(x, up_ref[...])).astype(BF16)
    out_ref[...] = dot(hidden, down_ref[...]).astype(out_ref.dtype)


def expert_apply(rows, w_gate, w_up, w_down, dtype, n_rows=None):
    n_rows, width = n_rows or rows.shape[0], rows.shape[1]
    hidden = w_gate.shape[1]
    tile = min(512, n_rows)
    return pl.pallas_call(
        expert_body,
        grid=(n_rows // tile,),
        in_specs=[
            pl.BlockSpec((tile, width), lambda i: (i, 0)),
            pl.BlockSpec((width, hidden), lambda i: (0, 0)),
            pl.BlockSpec((width, hidden), lambda i: (0, 0)),
            pl.BlockSpec((hidden, width), lambda i: (0, 0)),
        ],
        out_specs=pl.BlockSpec((tile, width), lambda i: (i, 0)),
        out_shape=jax.ShapeDtypeStruct((n_rows, width), dtype),
        cost_estimate=pl.CostEstimate(
            flops=6 * n_rows * width * hidden, bytes_accessed=14 << 20, transcendentals=0
        ),
        compiler_params=ALL_VMEM,
        name="expert",
    )(rows, w_gate, w_up, w_down)


def combine_body(weight_ref, rows_ref, shared_ref, out_ref):
    both = dot(weight_ref[...], rows_ref[...])
    n_tokens = out_ref.shape[0]
    out_ref[...] = (both[:n_tokens] + both[n_tokens:] + shared_ref[...]).astype(BF16)


def combine(weights, rows, shared):
    n_slots, width = rows.shape
    n_tokens = shared.shape[0]
    tile = width // 2
    return pl.pallas_call(
        combine_body,
        grid=(width // tile,),
        in_specs=[
            pl.BlockSpec((2 * n_tokens, n_slots), lambda i: (0, 0)),
            pl.BlockSpec((n_slots, tile), lambda i: (0, i)),
            pl.BlockSpec((n_tokens, tile), lambda i: (0, i)),
        ],
        out_specs=pl.BlockSpec((n_tokens, tile), lambda i: (0, i)),
        out_shape=jax.ShapeDtypeStruct((n_tokens, width), BF16),
        cost_estimate=pl.CostEstimate(
            flops=4 * n_tokens * n_slots * width, bytes_accessed=6 << 20, transcendentals=0
        ),
        compiler_params=ALL_VMEM,
        name="combine",
    )(weights, rows, shared)


def exchange(x, axes):
    return lax.all_to_all(x, axes, split_axis=0, concat_axis=0, tiled=True)


def local(
    query_rows,
    key_rows,
    value_rows,
    gate_rows,
    log_decay,
    out_proj,
    moe_input,
    norm_gain,
    routing,
    route_weight,
    expert_gate,
    expert_up,
    expert_down,
    shared_gate,
    shared_up,
    shared_down,
):
    n_rows = query_rows.shape[0]
    width = moe_input.shape[1]
    tp = lax.axis_size("tp")
    experts = lax.axis_size(EP) * tp

    n_tokens = moe_input.shape[0]
    places = lax.axis_size(EP)
    routes, route_weights = routing.T, route_weight.T
    message = norm(moe_input, norm_gain, routes)
    messages = all_shifts(message, "tp")

    keep, give = end_state(key_rows, value_rows, log_decay)
    got = shift(give, "ep_2", 1)
    pair = join_cores(keep, got)
    pairs = all_shifts(pair, "ep_1")
    before, plane = join_plane(pairs)
    planes = all_shifts(plane, "ep_0")
    mine, give = join_last(planes, before, keep, got)
    theirs = shift(give, "ep_2", 1)

    outgoing = dispatch(messages[:1], (0,), places)
    outgoing = dispatch(messages[1:], (1, 2, 3), places, outgoing)
    received = exchange(outgoing.reshape(places, tp * CAP, width), EP)

    own, other = gather_projection(out_proj)

    retained = mixer(query_rows, key_rows, value_rows, gate_rows, log_decay, mine, theirs)
    retained = retained.reshape(tp, n_rows // tp, -1)
    place = lax.axis_index("tp")
    heads = []
    for d in range(1, tp):
        block = lax.dynamic_index_in_dim(retained, (place + d) % tp, keepdims=False)
        heads.append(shift(block, "tp", d))

    shared = expert_apply(message, shared_gate, shared_up, shared_down, F32, n_tokens)
    weights = slot_weights(routes, route_weights, experts * CAP)

    served = expert_apply(
        received.reshape(-1, width), expert_gate[0], expert_up[0], expert_down[0], BF16
    )
    returned = exchange(served.reshape(experts, CAP, width), EP_TP)

    mixer_out = project(retained, heads, out_proj, own, other)
    moe_out = combine(weights, returned.reshape(-1, width), shared)
    return (mixer_out, moe_out)


def solution(mesh):
    split = Mesh(mesh.devices.reshape(4, 4, 2, mesh.shape["tp"]), ("ep_0", "ep_1", "ep_2", "tp"))
    return jax.shard_map(
        local,
        mesh=split,
        in_specs=(
            P(EP, "tp"),
            P(EP, "tp"),
            P(EP, "tp"),
            P(EP, "tp"),
            P("tp", EP),
            P("tp", None),
            P(EP_TP, None),
            P(),
            P(EP_TP, None),
            P(EP_TP, None),
            P(EP_TP, None, None),
            P(EP_TP, None, None),
            P(EP_TP, None, None),
            P(),
            P(),
            P(),
        ),
        out_specs=(P(EP_TP, None), P(EP_TP, None)),
        check_vma=False,
    )
```

```python
import functools

import jax
import jax.numpy as jnp
from jax import lax
from jax.experimental import pallas as pl
from jax.experimental.pallas import tpu as pltpu
from jax.sharding import Mesh
from jax.sharding import PartitionSpec as P


DK = 128
DV = 256
BLOCK = 128
CAP = 8
NOTE = 16
ROUTE = 8
EP = ("ep_0", "ep_1", "ep_2")
EP_TP = ("ep_0", "ep_1", "ep_2", "tp")
EPS = 1e-06
ALL_VMEM = pltpu.CompilerParams(vmem_limit_bytes=67043328)
SCALE = DK ** (-0.5)
F32 = jnp.float32
BF16 = jnp.bfloat16


def iota(shape, dim):
    return lax.broadcasted_iota(jnp.int32, shape, dim)


def dot(a, b):
    return jnp.dot(a, b, preferred_element_type=F32)


def dot_nt(a, b):
    return lax.dot_general(a, b, (((1,), (1,)), ((), ())), preferred_element_type=F32)


def dot_tn(a, b):
    return lax.dot_general(a, b, (((0,), (0,)), ((), ())), preferred_element_type=F32)


def silu(v):
    return v / (1.0 + jnp.exp(-v))


def thirds(a):
    high = a.astype(BF16)
    rest = a - high.astype(F32)
    middle = rest.astype(BF16)
    return high, middle, (rest - middle.astype(F32)).astype(BF16)


def sums_down(pick, a):
    return sum(dot_nt(pick, part) for part in thirds(a))


def sums_across(a, pick):
    return sum(dot(part, pick) for part in thirds(a))


def write_message(ref, state, total):
    whole = jnp.broadcast_to(total, (NOTE, DV))
    high, middle, low = (part.astype(F32) for part in thirds(whole))
    row = iota((NOTE, DV), 0)
    ref[:DK] = state.astype(BF16)
    ref[DK:] = jnp.where(row == 0, high, jnp.where(row == 1, middle, low)).astype(BF16)


def read_message(ref):
    note = ref[DK:].astype(F32)
    return ref[:DK].astype(F32), note[0:1] + note[1:2] + note[2:3]


def end_state_body(k_ref, v_ref, a_ref, keep_ref, give_ref, state, total):
    step = pl.program_id(0)

    @pl.when(step == 0)
    def _():
        state[...] = jnp.zeros_like(state)
        total[...] = jnp.zeros_like(total)

    n_heads = a_ref.shape[0]
    n_blocks = k_ref.shape[0] // BLOCK
    after = iota((BLOCK, BLOCK), 1) > iota((BLOCK, BLOCK), 0)
    pick = jnp.where(after, 1.0, 0.0).astype(BF16)
    later = jnp.zeros((n_heads, 1), F32)
    keys = [[] for _ in range(n_heads)]
    for b in reversed(range(n_blocks)):
        rows = pl.ds(b * BLOCK, BLOCK)
        a = a_ref[:, rows]
        left = sums_down(pick, a)
        for h in range(n_heads):
            k = k_ref[rows, h * DK : (h + 1) * DK].astype(F32)
            fade = SCALE * jnp.exp(left[:, h : h + 1] + later[h : h + 1, :])
            keys[h].insert(0, (k * fade).astype(BF16))
        later = later + jnp.sum(a, axis=1, keepdims=True)
    for h in range(n_heads):
        gone = later[h : h + 1, :]
        added = dot_tn(jnp.concatenate(keys[h], axis=0), v_ref[:, h * DV : (h + 1) * DV])
        state[h] = state[h] * jnp.exp(gone) + added
        total[h] = total[h] + gone

    @pl.when(step == pl.num_programs(0) - 1)
    def _():
        core = lax.axis_index("ep_2")
        write_message(keep_ref, state[core], total[core][0:1, 0:1])
        write_message(give_ref, state[1 - core], total[1 - core][0:1, 0:1])


def end_state(key_rows, value_rows, log_decay):
    n_rows, n_heads = key_rows.shape[0], log_decay.shape[0]
    tile = min(512, n_rows)
    return pl.pallas_call(
        end_state_body,
        grid=(n_rows // tile,),
        in_specs=[
            pl.BlockSpec((tile, n_heads * DK), lambda i: (i, 0)),
            pl.BlockSpec((tile, n_heads * DV), lambda i: (i, 0)),
            pl.BlockSpec((n_heads, tile), lambda i: (0, i)),
        ],
        out_specs=[pl.BlockSpec((DK + NOTE, DV), lambda i: (0, 0))] * 2,
        out_shape=[jax.ShapeDtypeStruct((DK + NOTE, DV), BF16)] * 2,
        scratch_shapes=[
            pltpu.VMEM((n_heads, DK, DV), F32),
            pltpu.VMEM((n_heads, 8, 128), F32),
        ],
        cost_estimate=pl.CostEstimate(
            flops=2 * n_rows * n_heads * DK * DV, bytes_accessed=4 << 20, transcendentals=0
        ),
        compiler_params=ALL_VMEM,
        name="end_state",
    )(key_rows, value_rows, log_decay)


def join_cores_body(keep_ref, got_ref, out_ref):
    core = lax.axis_index("ep_2")
    keep, kept = read_message(keep_ref)
    got, gone = read_message(got_ref)
    first = core == 0
    joined = jnp.where(first, keep * jnp.exp(gone) + got, got * jnp.exp(kept) + keep)
    write_message(out_ref, joined, kept + gone)


def join_cores(keep, got):
    return pl.pallas_call(
        join_cores_body,
        out_shape=jax.ShapeDtypeStruct(keep.shape, BF16),
        compiler_params=ALL_VMEM,
        name="join_cores",
    )(keep, got)


def join(axis, messages, ordered):
    peers, me = len(messages), lax.axis_index(axis)
    for d in range(peers):
        ordered[(me - d + peers) % peers] = messages[d][...]
    running, ahead = jnp.zeros((DK, DV), F32), jnp.zeros((DK, DV), F32)
    total, ahead_total = jnp.zeros((1, DV), F32), jnp.zeros((1, DV), F32)
    for k in range(peers):
        ahead = jnp.where(k == me, running, ahead)
        ahead_total = jnp.where(k == me, total, ahead_total)
        state, gone = read_message(ordered.at[k])
        running = running * jnp.exp(gone) + state
        total = total + gone
    return ahead, ahead_total, running, total


def join_plane_body(*refs):
    messages, (before_ref, all_ref, ordered) = refs[:-3], refs[-3:]
    ahead, gone, running, total = join("ep_1", messages, ordered)
    before_ref[:DK] = ahead
    before_ref[DK:] = jnp.broadcast_to(gone, (8, DV))
    write_message(all_ref, running, total)


def join_plane(messages):
    shape = messages[0].shape
    return pl.pallas_call(
        join_plane_body,
        out_shape=[
            jax.ShapeDtypeStruct((DK + 8, DV), F32),
            jax.ShapeDtypeStruct(shape, BF16),
        ],
        scratch_shapes=[pltpu.VMEM((len(messages),) + shape, BF16)],
        compiler_params=ALL_VMEM,
        cost_estimate=pl.CostEstimate(flops=1 << 22, bytes_accessed=1 << 20, transcendentals=0),
        name="join_plane",
    )(*messages)


def join_last_body(*refs):
    messages, (before_ref, keep_ref, got_ref, mine_ref, theirs_ref, ordered) = refs[:-6], refs[-6:]
    ahead, _, _, _ = join("ep_0", messages, ordered)
    gone = before_ref[DK : DK + 1]
    first = ahead * jnp.exp(gone) + before_ref[:DK]
    keep, kept = read_message(keep_ref)
    got, gone = read_message(got_ref)
    low = lax.axis_index("ep_2") == 0
    second = first * jnp.exp(jnp.where(low, kept, gone)) + jnp.where(low, keep, got)
    mine_ref[...] = jnp.where(low, first, second)
    theirs_ref[...] = jnp.where(low, second, first).astype(BF16)


def join_last(messages, before, keep, got):
    shape = messages[0].shape
    return pl.pallas_call(
        join_last_body,
        out_shape=[
            jax.ShapeDtypeStruct((DK, DV), F32),
            jax.ShapeDtypeStruct((DK, DV), BF16),
        ],
        scratch_shapes=[pltpu.VMEM((len(messages),) + shape, BF16)],
        compiler_params=ALL_VMEM,
        cost_estimate=pl.CostEstimate(flops=1 << 22, bytes_accessed=1 << 20, transcendentals=0),
        name="join_last",
    )(*messages, before, keep, got)


def shift(x, axis, d):
    peers = lax.axis_size(axis)
    return lax.ppermute(x, axis, [(k, (k + d) % peers) for k in range(peers)])


def all_shifts(x, axis):
    return [x] + [shift(x, axis, d) for d in range(1, lax.axis_size(axis))]


def mixer_body(q_ref, k_ref, v_ref, g_ref, a_ref, mine_ref, theirs_ref, out_ref, state):
    @pl.when(pl.program_id(0) == 0)
    def _():
        core = lax.axis_index("ep_2")
        state[core] = mine_ref[...]
        state[1 - core] = theirs_ref[...].astype(F32)

    n_heads = a_ref.shape[0]
    t, m = iota((BLOCK, BLOCK), 0), iota((BLOCK, BLOCK), 1)
    causal = t >= m
    upto = jnp.where(t <= m, 1.0, 0.0).astype(BF16)
    downto = jnp.where(causal, 1.0, 0.0).astype(BF16)
    for b in range(q_ref.shape[0] // BLOCK):
        rows = pl.ds(b * BLOCK, BLOCK)
        a = a_ref[:, rows]
        down = sums_down(downto, a)
        across = sums_across(a, upto)
        for h in range(n_heads):
            q = q_ref[rows, h * DK : (h + 1) * DK]
            k = k_ref[rows, h * DK : (h + 1) * DK]
            v = v_ref[rows, h * DV : (h + 1) * DV]
            gate = g_ref[rows, h * DV : (h + 1) * DV].astype(F32)
            col, row = down[:, h : h + 1], across[h : h + 1, :]
            whole = row[:, BLOCK - 1 : BLOCK]
            decay = jnp.where(causal, jnp.exp(jnp.where(causal, col - row, 0.0)), 0.0)
            weight = (dot_nt(q, k) * SCALE * decay).astype(BF16)
            before = state[h]
            raw = dot(weight, v) + dot(q, before.astype(BF16)) * jnp.exp(col)
            faded = (k.astype(F32) * (SCALE * jnp.exp(whole - col))).astype(BF16)
            state[h] = before * jnp.exp(whole) + dot_tn(faded, v)
            centered = raw - jnp.mean(raw, axis=1, keepdims=True)
            spread = jnp.mean(centered * centered, axis=1, keepdims=True)
            normed = centered * lax.rsqrt(spread + EPS)
            out_ref[rows, h * DV : (h + 1) * DV] = (silu(gate) * normed).astype(BF16)


def mixer(query_rows, key_rows, value_rows, gate_rows, log_decay, mine, theirs):
    n_rows, n_heads = query_rows.shape[0], log_decay.shape[0]
    tile = min(256, n_rows)
    return pl.pallas_call(
        mixer_body,
        grid=(n_rows // tile,),
        in_specs=[
            pl.BlockSpec((tile, n_heads * DK), lambda i: (i, 0)),
            pl.BlockSpec((tile, n_heads * DK), lambda i: (i, 0)),
            pl.BlockSpec((tile, n_heads * DV), lambda i: (i, 0)),
            pl.BlockSpec((tile, n_heads * DV), lambda i: (i, 0)),
            pl.BlockSpec((n_heads, tile), lambda i: (0, i)),
            pl.BlockSpec((DK, DV), lambda i: (0, 0)),
            pl.BlockSpec((DK, DV), lambda i: (0, 0)),
        ],
        out_specs=pl.BlockSpec((tile, n_heads * DV), lambda i: (i, 0)),
        out_shape=jax.ShapeDtypeStruct((n_rows, n_heads * DV), BF16),
        scratch_shapes=[pltpu.VMEM((n_heads, DK, DV), F32)],
        cost_estimate=pl.CostEstimate(
            flops=12 * n_rows * n_heads * DK * DV, bytes_accessed=8 << 20, transcendentals=0
        ),
        compiler_params=ALL_VMEM,
        name="mixer",
    )(query_rows, key_rows, value_rows, gate_rows, log_decay, mine, theirs)


def project_body(*refs):
    heads, whole, own, other, out_ref, lhs, rhs, sems = (
        refs[:4],
        refs[4],
        refs[5:9],
        refs[9:13],
        *refs[13:],
    )
    x, core = lax.axis_index("tp"), lax.axis_index("ep_2")
    half = rhs.shape[-1]
    pairs = [(heads[0].at[x], lhs.at[0])]
    for d in range(1, 4):
        pairs.append((heads[d], lhs.at[d]))
    for side in range(2):
        pairs.append((whole.at[:, side * half : (side + 1) * half], rhs.at[0, side]))
    cut = rhs.shape[2] // 2
    for parts, side in ((own, core), (other, 1 - core)):
        pairs.append((parts[0], rhs.at[1, side]))
        pairs.append((parts[1], rhs.at[2, side, :cut]))
        pairs.append((parts[2], rhs.at[2, side, cut:]))
        pairs.append((parts[3], rhs.at[3, side]))
    copies = [
        pltpu.make_async_copy(source, target, sems.at[n])
        for n, (source, target) in enumerate(pairs)
    ]
    for copy in copies:
        copy.start()
    for copy in copies:
        copy.wait()
    fine = half // 2
    for side in range(2):
        for part in range(2):
            at = slice(part * fine, (part + 1) * fine)
            total = dot(lhs[0], rhs[0, side, :, at])
            for d in range(1, 4):
                total = total + dot(lhs[d], rhs[d, side, :, at])
            start = side * half + part * fine
            out_ref[:, start : start + fine] = total.astype(BF16)


def project(retained, received, whole, own, other):
    groups, n_rows, width = retained.shape
    half = whole.shape[1] // 2
    arrays = [retained, *received, whole, *own, *other]
    return pl.pallas_call(
        project_body,
        in_specs=[pl.BlockSpec(memory_space=pl.ANY)] * len(arrays),
        out_shape=jax.ShapeDtypeStruct((n_rows, 2 * half), BF16),
        scratch_shapes=[
            pltpu.VMEM((groups, n_rows, width), BF16),
            pltpu.VMEM((groups, 2, width, half), BF16),
            pltpu.SemaphoreType.DMA((14,)),
        ],
        cost_estimate=pl.CostEstimate(
            flops=4 * n_rows * groups * width * half, bytes_accessed=12 << 20, transcendentals=0
        ),
        compiler_params=ALL_VMEM,
        name="project",
    )(*arrays)


def gather_projection(out_proj):
    n_rows, width = out_proj.shape
    half, cut = width // 2, n_rows // 2
    mine = lax.dynamic_slice(out_proj, (0, lax.axis_index("ep_2") * half), (n_rows, half))
    below, above = shift(mine, "tp", 1), shift(mine, "tp", 3)
    far = [shift(below[:cut], "tp", 1), shift(above[cut:], "tp", 3)]
    own = [below, *far, above]
    other = [shift(part, "ep_2", 1) for part in own]
    return own, other


def norm_body(x_ref, gain_ref, route_ref, out_ref):
    x = x_ref[...].astype(F32)
    n_tokens = x.shape[0]
    mean = jnp.mean(x * x, axis=1, keepdims=True)
    out_ref[:n_tokens] = (x * lax.rsqrt(mean + EPS) * gain_ref[...]).astype(BF16)
    row = iota((ROUTE, n_tokens), 0)
    note = jnp.zeros((ROUTE, n_tokens), F32)
    for k in range(route_ref.shape[0]):
        note = jnp.where(row == k, route_ref[k : k + 1].astype(F32), note)
    out_ref[n_tokens:, :n_tokens] = note.astype(BF16)
    rest = (ROUTE, x.shape[1] - n_tokens)
    out_ref[n_tokens:, n_tokens:] = jnp.zeros(rest, BF16)


def norm(moe_input, norm_gain, routes):
    n_tokens, width = moe_input.shape
    return pl.pallas_call(
        norm_body,
        out_shape=jax.ShapeDtypeStruct((n_tokens + ROUTE, width), BF16),
        compiler_params=ALL_VMEM,
        name="norm",
    )(moe_input, norm_gain.reshape(1, width), routes)


def ranked(hits, n_tokens, none=float(CAP)):
    earlier = iota((n_tokens, n_tokens), 0) < iota((n_tokens, n_tokens), 1)
    rank = dot(hits.astype(BF16), jnp.where(earlier, 1.0, 0.0).astype(BF16))
    return jnp.where(hits > 0.0, rank, none).astype(BF16)


def slot_owners(n_slots):
    shape = (n_slots, n_slots // CAP)
    return jnp.where(iota(shape, 0) // CAP == iota(shape, 1), 1.0, 0.0).astype(BF16)


def picks_of(note, n_slots):
    n_tokens = note.shape[1]
    experts = n_slots // CAP
    line = lax.axis_size("tp")
    expert = (iota((experts, n_tokens), 0) * line + lax.axis_index("tp")).astype(F32)
    hits = jnp.zeros((experts, n_tokens), F32)
    for k in range(4):
        hits = jnp.where(note[k : k + 1] == expert, 1.0, hits)
    place = (iota((n_slots, n_tokens), 0) & (CAP - 1)).astype(F32)
    here = dot(slot_owners(n_slots), ranked(hits, n_tokens)) == place
    return jnp.where(here, 1.0, 0.0).astype(BF16)


def dispatch_body(shifts, *refs):
    n = len(shifts)
    messages, (out_ref, held, made, sems) = refs[:n], refs[-4:]
    experts, line, _, width = out_ref.shape
    n_tokens = held.shape[1] - ROUTE
    me = lax.axis_index("tp")
    arrive, leave = [], []
    for i, d in enumerate(shifts):
        to = out_ref.at[:, (me - d + line) % line]
        arrive.append(pltpu.make_async_copy(messages[i], held.at[i], sems.at[0, i]))
        leave.append(pltpu.make_async_copy(made.at[i], to, sems.at[1, i]))
    for copy in arrive:
        copy.start()
    for i in range(n):
        arrive[i].wait()
        pick = picks_of(held[i, n_tokens:, :n_tokens].astype(F32), experts * CAP)
        rows = dot(pick, held[i, :n_tokens])
        made[i] = rows.reshape(experts, CAP, width).astype(BF16)
        leave[i].start()
    for copy in leave:
        copy.wait()


def dispatch(messages, shifts, experts, outgoing=None):
    n, (n_rows, width) = len(messages), messages[0].shape
    arrays = list(messages) + ([] if outgoing is None else [outgoing])
    shape = (experts, lax.axis_size("tp"), CAP, width)
    return pl.pallas_call(
        functools.partial(dispatch_body, shifts),
        in_specs=[pl.BlockSpec(memory_space=pl.ANY)] * len(arrays),
        out_specs=pl.BlockSpec(memory_space=pl.ANY),
        out_shape=jax.ShapeDtypeStruct(shape, BF16),
        scratch_shapes=[
            pltpu.VMEM((n, n_rows, width), BF16),
            pltpu.VMEM((n, experts, CAP, width), BF16),
            pltpu.SemaphoreType.DMA((2, n)),
        ],
        input_output_aliases={} if outgoing is None else {n: 0},
        compiler_params=ALL_VMEM,
        cost_estimate=pl.CostEstimate(
            flops=256 * n * experts * CAP * width, bytes_accessed=2 * n << 20, transcendentals=0
        ),
        name="dispatch",
    )(*arrays)


def weights_body(route_ref, weight_ref, out_ref):
    n_visits, n_tokens = route_ref.shape
    n_slots = out_ref.shape[1]
    experts = n_slots // CAP
    expert = iota((experts, n_tokens), 0)
    hits = jnp.zeros((experts, n_tokens), F32)
    weighed = jnp.zeros((experts, n_tokens), F32)
    for k in range(n_visits):
        hit = route_ref[k : k + 1] == expert
        hits = jnp.where(hit, 1.0, hits)
        weighed = jnp.where(hit, weight_ref[k : k + 1], weighed)
    spread = jnp.where(iota((n_slots, experts), 0) // CAP == iota((n_slots, experts), 1), 1.0, 0.0)
    spread = spread.astype(BF16)
    place = (iota((n_slots, n_tokens), 0) % CAP).astype(F32)
    here = dot(spread, ranked(hits, n_tokens)) == place
    high = weighed.astype(BF16)
    low = (weighed - high.astype(F32)).astype(BF16)
    out_ref[:n_tokens] = jnp.where(here, dot(spread, high), 0.0).T.astype(BF16)
    out_ref[n_tokens:] = jnp.where(here, dot(spread, low), 0.0).T.astype(BF16)


def slot_weights(routes, route_weights, n_slots):
    n_tokens = routes.shape[1]
    return pl.pallas_call(
        weights_body,
        out_shape=jax.ShapeDtypeStruct((2 * n_tokens, n_slots), BF16),
        compiler_params=ALL_VMEM,
        cost_estimate=pl.CostEstimate(flops=1 << 27, bytes_accessed=1 << 20, transcendentals=0),
        name="weights",
    )(routes, route_weights)


def expert_body(x_ref, gate_ref, up_ref, down_ref, out_ref):
    x = x_ref[...]
    hidden = (silu(dot(x, gate_ref[...])) * dot(x, up_ref[...])).astype(BF16)
    out_ref[...] = dot(hidden, down_ref[...]).astype(out_ref.dtype)


def expert_held(rows, w_gate, w_up, w_down):
    n_rows, width = rows.shape
    hidden = w_gate.shape[1]
    tile = 256
    w_gate = pltpu.with_memory_space_constraint(w_gate, pltpu.VMEM)
    return pl.pallas_call(
        expert_body,
        grid=(n_rows // tile,),
        in_specs=[
            pl.BlockSpec((tile, width), lambda i: (i, 0)),
            pl.BlockSpec(memory_space=pltpu.VMEM),
            pl.BlockSpec((width, hidden), lambda i: (0, 0)),
            pl.BlockSpec((hidden, width), lambda i: (0, 0)),
        ],
        out_specs=pl.BlockSpec((tile, width), lambda i: (i, 0)),
        out_shape=jax.ShapeDtypeStruct((n_rows, width), BF16),
        compiler_params=pltpu.CompilerParams(vmem_limit_bytes=62500000),
        cost_estimate=pl.CostEstimate(
            flops=6 * n_rows * width * hidden, bytes_accessed=12 << 20, transcendentals=0
        ),
        name="expert",
    )(rows, w_gate, w_up, w_down)


def expert_apply(rows, w_gate, w_up, w_down, dtype, n_rows=None):
    n_rows, width = n_rows or rows.shape[0], rows.shape[1]
    hidden = w_gate.shape[1]
    tile = min(512, n_rows)
    return pl.pallas_call(
        expert_body,
        grid=(n_rows // tile,),
        in_specs=[
            pl.BlockSpec((tile, width), lambda i: (i, 0)),
            pl.BlockSpec((width, hidden), lambda i: (0, 0)),
            pl.BlockSpec((width, hidden), lambda i: (0, 0)),
            pl.BlockSpec((hidden, width), lambda i: (0, 0)),
        ],
        out_specs=pl.BlockSpec((tile, width), lambda i: (i, 0)),
        out_shape=jax.ShapeDtypeStruct((n_rows, width), dtype),
        cost_estimate=pl.CostEstimate(
            flops=6 * n_rows * width * hidden, bytes_accessed=14 << 20, transcendentals=0
        ),
        compiler_params=ALL_VMEM,
        name="expert",
    )(rows, w_gate, w_up, w_down)


def combine_body(weight_ref, rows_ref, shared_ref, out_ref):
    both = dot(weight_ref[...], rows_ref[...])
    n_tokens = out_ref.shape[0]
    out_ref[...] = (both[:n_tokens] + both[n_tokens:] + shared_ref[...]).astype(BF16)


def combine(weights, rows, shared):
    n_slots, width = rows.shape
    n_tokens = shared.shape[0]
    tile = width // 2
    return pl.pallas_call(
        combine_body,
        grid=(width // tile,),
        in_specs=[
            pl.BlockSpec((2 * n_tokens, n_slots), lambda i: (0, 0)),
            pl.BlockSpec((n_slots, tile), lambda i: (0, i)),
            pl.BlockSpec((n_tokens, tile), lambda i: (0, i)),
        ],
        out_specs=pl.BlockSpec((n_tokens, tile), lambda i: (0, i)),
        out_shape=jax.ShapeDtypeStruct((n_tokens, width), BF16),
        cost_estimate=pl.CostEstimate(
            flops=4 * n_tokens * n_slots * width, bytes_accessed=6 << 20, transcendentals=0
        ),
        compiler_params=ALL_VMEM,
        name="combine",
    )(weights, rows, shared)


def exchange(x, axes):
    return lax.all_to_all(x, axes, split_axis=0, concat_axis=0, tiled=True)


def local(
    query_rows,
    key_rows,
    value_rows,
    gate_rows,
    log_decay,
    out_proj,
    moe_input,
    norm_gain,
    routing,
    route_weight,
    expert_gate,
    expert_up,
    expert_down,
    shared_gate,
    shared_up,
    shared_down,
):
    n_rows = query_rows.shape[0]
    width = moe_input.shape[1]
    tp = lax.axis_size("tp")
    experts = lax.axis_size(EP) * tp

    n_tokens = moe_input.shape[0]
    places = lax.axis_size(EP)
    routes, route_weights = routing.T, route_weight.T
    message = norm(moe_input, norm_gain, routes)
    messages = all_shifts(message, "tp")

    keep, give = end_state(key_rows, value_rows, log_decay)
    got = shift(give, "ep_2", 1)
    pair = join_cores(keep, got)
    pairs = all_shifts(pair, "ep_1")
    before, plane = join_plane(pairs)
    planes = all_shifts(plane, "ep_0")
    mine, give = join_last(planes, before, keep, got)
    theirs = shift(give, "ep_2", 1)

    outgoing = dispatch(messages[:1], (0,), places)
    outgoing = dispatch(messages[1:], (1, 2, 3), places, outgoing)
    received = exchange(outgoing.reshape(places, tp * CAP, width), EP)

    own, other = gather_projection(out_proj)

    retained = mixer(query_rows, key_rows, value_rows, gate_rows, log_decay, mine, theirs)
    retained = retained.reshape(tp, n_rows // tp, -1)
    place = lax.axis_index("tp")
    heads = []
    for d in range(1, tp):
        block = lax.dynamic_index_in_dim(retained, (place + d) % tp, keepdims=False)
        heads.append(shift(block, "tp", d))

    shared = expert_apply(message, shared_gate, shared_up, shared_down, F32, n_tokens)
    weights = slot_weights(routes, route_weights, experts * CAP)

    served = expert_held(received.reshape(-1, width), expert_gate[0], expert_up[0], expert_down[0])
    returned = exchange(served.reshape(experts, CAP, width), EP_TP)

    mixer_out = project(retained, heads, out_proj, own, other)
    moe_out = combine(weights, returned.reshape(-1, width), shared)
    return (mixer_out, moe_out)


def solution(mesh):
    split = Mesh(mesh.devices.reshape(4, 4, 2, mesh.shape["tp"]), ("ep_0", "ep_1", "ep_2", "tp"))
    return jax.shard_map(
        local,
        mesh=split,
        in_specs=(
            P(EP, "tp"),
            P(EP, "tp"),
            P(EP, "tp"),
            P(EP, "tp"),
            P("tp", EP),
            P("tp", None),
            P(EP_TP, None),
            P(),
            P(EP_TP, None),
            P(EP_TP, None),
            P(EP_TP, None, None),
            P(EP_TP, None, None),
            P(EP_TP, None, None),
            P(),
            P(),
            P(),
        ),
        out_specs=(P(EP_TP, None), P(EP_TP, None)),
        check_vma=False,
    )
```

```python
import functools

import jax
import jax.numpy as jnp
from jax import lax
from jax.experimental import pallas as pl
from jax.experimental.pallas import tpu as pltpu
from jax.sharding import Mesh
from jax.sharding import PartitionSpec as P


DK = 128
DV = 256
BLOCK = 128
CAP = 8
NOTE = 16
ROUTE = 8
EP = ("ep_0", "ep_1", "ep_2")
EP_TP = ("ep_0", "ep_1", "ep_2", "tp")
EPS = 1e-06
ALL_VMEM = pltpu.CompilerParams(vmem_limit_bytes=67043328)
SCALE = DK ** (-0.5)
F32 = jnp.float32
BF16 = jnp.bfloat16


def iota(shape, dim):
    return lax.broadcasted_iota(jnp.int32, shape, dim)


def dot(a, b):
    return jnp.dot(a, b, preferred_element_type=F32)


def dot_nt(a, b):
    return lax.dot_general(a, b, (((1,), (1,)), ((), ())), preferred_element_type=F32)


def dot_tn(a, b):
    return lax.dot_general(a, b, (((0,), (0,)), ((), ())), preferred_element_type=F32)


def silu(v):
    return v / (1.0 + jnp.exp(-v))


def thirds(a):
    high = a.astype(BF16)
    rest = a - high.astype(F32)
    middle = rest.astype(BF16)
    return high, middle, (rest - middle.astype(F32)).astype(BF16)


def sums_down(pick, a):
    return sum(dot_nt(pick, part) for part in thirds(a))


def sums_across(a, pick):
    return sum(dot(part, pick) for part in thirds(a))


def write_message(ref, state, total):
    whole = jnp.broadcast_to(total, (NOTE, DV))
    high, middle, low = (part.astype(F32) for part in thirds(whole))
    row = iota((NOTE, DV), 0)
    ref[:DK] = state.astype(BF16)
    ref[DK:] = jnp.where(row == 0, high, jnp.where(row == 1, middle, low)).astype(BF16)


def read_message(ref):
    note = ref[DK:].astype(F32)
    return ref[:DK].astype(F32), note[0:1] + note[1:2] + note[2:3]


def end_state_body(k_ref, v_ref, a_ref, keep_ref, give_ref, state, total):
    step = pl.program_id(0)

    @pl.when(step == 0)
    def _():
        state[...] = jnp.zeros_like(state)
        total[...] = jnp.zeros_like(total)

    n_heads = a_ref.shape[0]
    n_blocks = k_ref.shape[0] // BLOCK
    after = iota((BLOCK, BLOCK), 1) > iota((BLOCK, BLOCK), 0)
    pick = jnp.where(after, 1.0, 0.0).astype(BF16)
    later = jnp.zeros((n_heads, 1), F32)
    keys = [[] for _ in range(n_heads)]
    for b in reversed(range(n_blocks)):
        rows = pl.ds(b * BLOCK, BLOCK)
        a = a_ref[:, rows]
        left = sums_down(pick, a)
        for h in range(n_heads):
            k = k_ref[rows, h * DK : (h + 1) * DK].astype(F32)
            fade = SCALE * jnp.exp(left[:, h : h + 1] + later[h : h + 1, :])
            keys[h].insert(0, (k * fade).astype(BF16))
        later = later + jnp.sum(a, axis=1, keepdims=True)
    for h in range(n_heads):
        gone = later[h : h + 1, :]
        added = dot_tn(jnp.concatenate(keys[h], axis=0), v_ref[:, h * DV : (h + 1) * DV])
        state[h] = state[h] * jnp.exp(gone) + added
        total[h] = total[h] + gone

    @pl.when(step == pl.num_programs(0) - 1)
    def _():
        core = lax.axis_index("ep_2")
        write_message(keep_ref, state[core], total[core][0:1, 0:1])
        write_message(give_ref, state[1 - core], total[1 - core][0:1, 0:1])


def end_state(key_rows, value_rows, log_decay):
    n_rows, n_heads = key_rows.shape[0], log_decay.shape[0]
    tile = min(512, n_rows)
    return pl.pallas_call(
        end_state_body,
        grid=(n_rows // tile,),
        in_specs=[
            pl.BlockSpec((tile, n_heads * DK), lambda i: (i, 0)),
            pl.BlockSpec((tile, n_heads * DV), lambda i: (i, 0)),
            pl.BlockSpec((n_heads, tile), lambda i: (0, i)),
        ],
        out_specs=[pl.BlockSpec((DK + NOTE, DV), lambda i: (0, 0))] * 2,
        out_shape=[jax.ShapeDtypeStruct((DK + NOTE, DV), BF16)] * 2,
        scratch_shapes=[
            pltpu.VMEM((n_heads, DK, DV), F32),
            pltpu.VMEM((n_heads, 8, 128), F32),
        ],
        cost_estimate=pl.CostEstimate(
            flops=2 * n_rows * n_heads * DK * DV, bytes_accessed=4 << 20, transcendentals=0
        ),
        compiler_params=ALL_VMEM,
        name="end_state",
    )(key_rows, value_rows, log_decay)


def join_cores_body(keep_ref, got_ref, out_ref):
    core = lax.axis_index("ep_2")
    keep, kept = read_message(keep_ref)
    got, gone = read_message(got_ref)
    first = core == 0
    joined = jnp.where(first, keep * jnp.exp(gone) + got, got * jnp.exp(kept) + keep)
    write_message(out_ref, joined, kept + gone)


def join_cores(keep, got):
    return pl.pallas_call(
        join_cores_body,
        out_shape=jax.ShapeDtypeStruct(keep.shape, BF16),
        compiler_params=ALL_VMEM,
        name="join_cores",
    )(keep, got)


def join(axis, messages, ordered):
    peers, me = len(messages), lax.axis_index(axis)
    for d in range(peers):
        ordered[(me - d + peers) % peers] = messages[d][...]
    running, ahead = jnp.zeros((DK, DV), F32), jnp.zeros((DK, DV), F32)
    total, ahead_total = jnp.zeros((1, DV), F32), jnp.zeros((1, DV), F32)
    for k in range(peers):
        ahead = jnp.where(k == me, running, ahead)
        ahead_total = jnp.where(k == me, total, ahead_total)
        state, gone = read_message(ordered.at[k])
        running = running * jnp.exp(gone) + state
        total = total + gone
    return ahead, ahead_total, running, total


def join_plane_body(*refs):
    messages, (before_ref, all_ref, ordered) = refs[:-3], refs[-3:]
    ahead, gone, running, total = join("ep_1", messages, ordered)
    before_ref[:DK] = ahead
    before_ref[DK:] = jnp.broadcast_to(gone, (8, DV))
    write_message(all_ref, running, total)


def join_plane(messages):
    shape = messages[0].shape
    return pl.pallas_call(
        join_plane_body,
        out_shape=[
            jax.ShapeDtypeStruct((DK + 8, DV), F32),
            jax.ShapeDtypeStruct(shape, BF16),
        ],
        scratch_shapes=[pltpu.VMEM((len(messages),) + shape, BF16)],
        compiler_params=ALL_VMEM,
        cost_estimate=pl.CostEstimate(flops=1 << 22, bytes_accessed=1 << 20, transcendentals=0),
        name="join_plane",
    )(*messages)


def join_last_body(*refs):
    messages, (before_ref, keep_ref, got_ref, mine_ref, theirs_ref, ordered) = refs[:-6], refs[-6:]
    ahead, _, _, _ = join("ep_0", messages, ordered)
    gone = before_ref[DK : DK + 1]
    first = ahead * jnp.exp(gone) + before_ref[:DK]
    keep, kept = read_message(keep_ref)
    got, gone = read_message(got_ref)
    low = lax.axis_index("ep_2") == 0
    second = first * jnp.exp(jnp.where(low, kept, gone)) + jnp.where(low, keep, got)
    mine_ref[...] = jnp.where(low, first, second)
    theirs_ref[...] = jnp.where(low, second, first).astype(BF16)


def join_last(messages, before, keep, got):
    shape = messages[0].shape
    return pl.pallas_call(
        join_last_body,
        out_shape=[
            jax.ShapeDtypeStruct((DK, DV), F32),
            jax.ShapeDtypeStruct((DK, DV), BF16),
        ],
        scratch_shapes=[pltpu.VMEM((len(messages),) + shape, BF16)],
        compiler_params=ALL_VMEM,
        cost_estimate=pl.CostEstimate(flops=1 << 22, bytes_accessed=1 << 20, transcendentals=0),
        name="join_last",
    )(*messages, before, keep, got)


def shift(x, axis, d):
    peers = lax.axis_size(axis)
    return lax.ppermute(x, axis, [(k, (k + d) % peers) for k in range(peers)])


def all_shifts(x, axis):
    return [x] + [shift(x, axis, d) for d in range(1, lax.axis_size(axis))]


def mixer_body(q_ref, k_ref, v_ref, g_ref, a_ref, mine_ref, theirs_ref, out_ref, state):
    @pl.when(pl.program_id(0) == 0)
    def _():
        core = lax.axis_index("ep_2")
        state[core] = mine_ref[...]
        state[1 - core] = theirs_ref[...].astype(F32)

    n_heads = a_ref.shape[0]
    t, m = iota((BLOCK, BLOCK), 0), iota((BLOCK, BLOCK), 1)
    causal = t >= m
    upto = jnp.where(t <= m, 1.0, 0.0).astype(BF16)
    downto = jnp.where(causal, 1.0, 0.0).astype(BF16)
    for b in range(q_ref.shape[0] // BLOCK):
        rows = pl.ds(b * BLOCK, BLOCK)
        a = a_ref[:, rows]
        down = sums_down(downto, a)
        across = sums_across(a, upto)
        for h in range(n_heads):
            q = q_ref[rows, h * DK : (h + 1) * DK]
            k = k_ref[rows, h * DK : (h + 1) * DK]
            v = v_ref[rows, h * DV : (h + 1) * DV]
            gate = g_ref[rows, h * DV : (h + 1) * DV].astype(F32)
            col, row = down[:, h : h + 1], across[h : h + 1, :]
            whole = row[:, BLOCK - 1 : BLOCK]
            decay = jnp.where(causal, jnp.exp(jnp.where(causal, col - row, 0.0)), 0.0)
            weight = (dot_nt(q, k) * SCALE * decay).astype(BF16)
            before = state[h]
            raw = dot(weight, v) + dot(q, before.astype(BF16)) * jnp.exp(col)
            faded = (k.astype(F32) * (SCALE * jnp.exp(whole - col))).astype(BF16)
            state[h] = before * jnp.exp(whole) + dot_tn(faded, v)
            centered = raw - jnp.mean(raw, axis=1, keepdims=True)
            spread = jnp.mean(centered * centered, axis=1, keepdims=True)
            normed = centered * lax.rsqrt(spread + EPS)
            out_ref[rows, h * DV : (h + 1) * DV] = (silu(gate) * normed).astype(BF16)


def mixer(query_rows, key_rows, value_rows, gate_rows, log_decay, mine, theirs):
    n_rows, n_heads = query_rows.shape[0], log_decay.shape[0]
    tile = min(256, n_rows)
    return pl.pallas_call(
        mixer_body,
        grid=(n_rows // tile,),
        in_specs=[
            pl.BlockSpec((tile, n_heads * DK), lambda i: (i, 0)),
            pl.BlockSpec((tile, n_heads * DK), lambda i: (i, 0)),
            pl.BlockSpec((tile, n_heads * DV), lambda i: (i, 0)),
            pl.BlockSpec((tile, n_heads * DV), lambda i: (i, 0)),
            pl.BlockSpec((n_heads, tile), lambda i: (0, i)),
            pl.BlockSpec((DK, DV), lambda i: (0, 0)),
            pl.BlockSpec((DK, DV), lambda i: (0, 0)),
        ],
        out_specs=pl.BlockSpec((tile, n_heads * DV), lambda i: (i, 0)),
        out_shape=jax.ShapeDtypeStruct((n_rows, n_heads * DV), BF16),
        scratch_shapes=[pltpu.VMEM((n_heads, DK, DV), F32)],
        cost_estimate=pl.CostEstimate(
            flops=12 * n_rows * n_heads * DK * DV, bytes_accessed=8 << 20, transcendentals=0
        ),
        compiler_params=ALL_VMEM,
        name="mixer",
    )(query_rows, key_rows, value_rows, gate_rows, log_decay, mine, theirs)


def project_body(*refs):
    heads, whole, own, other, out_ref, lhs, rhs, sems = (
        refs[:4],
        refs[4],
        refs[5:9],
        refs[9:13],
        *refs[13:],
    )
    x, core = lax.axis_index("tp"), lax.axis_index("ep_2")
    half = rhs.shape[-1]
    pairs = [(heads[0].at[x], lhs.at[0])]
    for d in range(1, 4):
        pairs.append((heads[d], lhs.at[d]))
    for side in range(2):
        pairs.append((whole.at[:, side * half : (side + 1) * half], rhs.at[0, side]))
    cut = rhs.shape[2] // 2
    for parts, side in ((own, core), (other, 1 - core)):
        pairs.append((parts[0], rhs.at[1, side]))
        pairs.append((parts[1], rhs.at[2, side, :cut]))
        pairs.append((parts[2], rhs.at[2, side, cut:]))
        pairs.append((parts[3], rhs.at[3, side]))
    copies = [
        pltpu.make_async_copy(source, target, sems.at[n])
        for n, (source, target) in enumerate(pairs)
    ]
    for copy in copies:
        copy.start()
    for copy in copies:
        copy.wait()
    fine = half // 2
    for side in range(2):
        for part in range(2):
            at = slice(part * fine, (part + 1) * fine)
            total = dot(lhs[0], rhs[0, side, :, at])
            for d in range(1, 4):
                total = total + dot(lhs[d], rhs[d, side, :, at])
            start = side * half + part * fine
            out_ref[:, start : start + fine] = total.astype(BF16)


def project(retained, received, whole, own, other):
    groups, n_rows, width = retained.shape
    half = whole.shape[1] // 2
    arrays = [retained, *received, whole, *own, *other]
    return pl.pallas_call(
        project_body,
        in_specs=[pl.BlockSpec(memory_space=pl.ANY)] * len(arrays),
        out_shape=jax.ShapeDtypeStruct((n_rows, 2 * half), BF16),
        scratch_shapes=[
            pltpu.VMEM((groups, n_rows, width), BF16),
            pltpu.VMEM((groups, 2, width, half), BF16),
            pltpu.SemaphoreType.DMA((14,)),
        ],
        cost_estimate=pl.CostEstimate(
            flops=4 * n_rows * groups * width * half, bytes_accessed=12 << 20, transcendentals=0
        ),
        compiler_params=ALL_VMEM,
        name="project",
    )(*arrays)


def gather_projection(out_proj):
    n_rows, width = out_proj.shape
    half, cut = width // 2, n_rows // 2
    mine = lax.dynamic_slice(out_proj, (0, lax.axis_index("ep_2") * half), (n_rows, half))
    below, above = shift(mine, "tp", 1), shift(mine, "tp", 3)
    far = [shift(below[:cut], "tp", 1), shift(above[cut:], "tp", 3)]
    own = [below, *far, above]
    other = [shift(part, "ep_2", 1) for part in own]
    return own, other


def norm_body(x_ref, gain_ref, route_ref, out_ref):
    x = x_ref[...].astype(F32)
    n_tokens = x.shape[0]
    mean = jnp.mean(x * x, axis=1, keepdims=True)
    out_ref[:n_tokens] = (x * lax.rsqrt(mean + EPS) * gain_ref[...]).astype(BF16)
    row = iota((ROUTE, n_tokens), 0)
    note = jnp.zeros((ROUTE, n_tokens), F32)
    for k in range(route_ref.shape[0]):
        note = jnp.where(row == k, route_ref[k : k + 1].astype(F32), note)
    out_ref[n_tokens:, :n_tokens] = note.astype(BF16)
    rest = (ROUTE, x.shape[1] - n_tokens)
    out_ref[n_tokens:, n_tokens:] = jnp.zeros(rest, BF16)


def norm(moe_input, norm_gain, routes):
    n_tokens, width = moe_input.shape
    return pl.pallas_call(
        norm_body,
        out_shape=jax.ShapeDtypeStruct((n_tokens + ROUTE, width), BF16),
        compiler_params=ALL_VMEM,
        name="norm",
    )(moe_input, norm_gain.reshape(1, width), routes)


def ranked(hits, n_tokens, none=float(CAP)):
    earlier = iota((n_tokens, n_tokens), 0) < iota((n_tokens, n_tokens), 1)
    rank = dot(hits.astype(BF16), jnp.where(earlier, 1.0, 0.0).astype(BF16))
    return jnp.where(hits > 0.0, rank, none).astype(BF16)


def slot_owners(n_slots):
    shape = (n_slots, n_slots // CAP)
    return jnp.where(iota(shape, 0) // CAP == iota(shape, 1), 1.0, 0.0).astype(BF16)


def picks_of(note, n_slots):
    n_tokens = note.shape[1]
    experts = n_slots // CAP
    line = lax.axis_size("tp")
    expert = (iota((experts, n_tokens), 0) * line + lax.axis_index("tp")).astype(F32)
    hits = jnp.zeros((experts, n_tokens), F32)
    for k in range(4):
        hits = jnp.where(note[k : k + 1] == expert, 1.0, hits)
    place = (iota((n_slots, n_tokens), 0) & (CAP - 1)).astype(F32)
    here = dot(slot_owners(n_slots), ranked(hits, n_tokens)) == place
    return jnp.where(here, 1.0, 0.0).astype(BF16)


def dispatch_body(shifts, *refs):
    n = len(shifts)
    messages, (out_ref, held, made, sems) = refs[:n], refs[-4:]
    experts, line, _, width = out_ref.shape
    n_tokens = held.shape[1] - ROUTE
    me = lax.axis_index("tp")
    arrive, leave = [], []
    for i, d in enumerate(shifts):
        to = out_ref.at[:, (me - d + line) % line]
        arrive.append(pltpu.make_async_copy(messages[i], held.at[i], sems.at[0, i]))
        leave.append(pltpu.make_async_copy(made.at[i], to, sems.at[1, i]))
    for copy in arrive:
        copy.start()
    for i in range(n):
        arrive[i].wait()
        pick = picks_of(held[i, n_tokens:, :n_tokens].astype(F32), experts * CAP)
        rows = dot(pick, held[i, :n_tokens])
        made[i] = rows.reshape(experts, CAP, width).astype(BF16)
        leave[i].start()
    for copy in leave:
        copy.wait()


def dispatch(messages, shifts, experts, outgoing=None):
    n, (n_rows, width) = len(messages), messages[0].shape
    arrays = list(messages) + ([] if outgoing is None else [outgoing])
    shape = (experts, lax.axis_size("tp"), CAP, width)
    return pl.pallas_call(
        functools.partial(dispatch_body, shifts),
        in_specs=[pl.BlockSpec(memory_space=pl.ANY)] * len(arrays),
        out_specs=pl.BlockSpec(memory_space=pl.ANY),
        out_shape=jax.ShapeDtypeStruct(shape, BF16),
        scratch_shapes=[
            pltpu.VMEM((n, n_rows, width), BF16),
            pltpu.VMEM((n, experts, CAP, width), BF16),
            pltpu.SemaphoreType.DMA((2, n)),
        ],
        input_output_aliases={} if outgoing is None else {n: 0},
        compiler_params=ALL_VMEM,
        cost_estimate=pl.CostEstimate(
            flops=256 * n * experts * CAP * width, bytes_accessed=2 * n << 20, transcendentals=0
        ),
        name="dispatch",
    )(*arrays)


def weights_body(route_ref, weight_ref, out_ref):
    n_visits, n_tokens = route_ref.shape
    n_slots = out_ref.shape[1]
    experts = n_slots // CAP
    expert = iota((experts, n_tokens), 0)
    hits = jnp.zeros((experts, n_tokens), F32)
    weighed = jnp.zeros((experts, n_tokens), F32)
    for k in range(n_visits):
        hit = route_ref[k : k + 1] == expert
        hits = jnp.where(hit, 1.0, hits)
        weighed = jnp.where(hit, weight_ref[k : k + 1], weighed)
    spread = jnp.where(iota((n_slots, experts), 0) // CAP == iota((n_slots, experts), 1), 1.0, 0.0)
    spread = spread.astype(BF16)
    place = (iota((n_slots, n_tokens), 0) % CAP).astype(F32)
    here = dot(spread, ranked(hits, n_tokens)) == place
    high = weighed.astype(BF16)
    low = (weighed - high.astype(F32)).astype(BF16)
    out_ref[:n_tokens] = jnp.where(here, dot(spread, high), 0.0).T.astype(BF16)
    out_ref[n_tokens:] = jnp.where(here, dot(spread, low), 0.0).T.astype(BF16)


def slot_weights(routes, route_weights, n_slots):
    n_tokens = routes.shape[1]
    return pl.pallas_call(
        weights_body,
        out_shape=jax.ShapeDtypeStruct((2 * n_tokens, n_slots), BF16),
        compiler_params=ALL_VMEM,
        cost_estimate=pl.CostEstimate(flops=1 << 27, bytes_accessed=1 << 20, transcendentals=0),
        name="weights",
    )(routes, route_weights)


def expert_body(x_ref, gate_ref, up_ref, down_ref, out_ref):
    x = x_ref[...]
    hidden = (silu(dot(x, gate_ref[...])) * dot(x, up_ref[...])).astype(BF16)
    out_ref[...] = dot(hidden, down_ref[...]).astype(out_ref.dtype)


def expert_held(rows, w_gate, w_up, w_down):
    n_rows, width = rows.shape
    hidden = w_gate.shape[1]
    tile = 256
    w_gate = pltpu.with_memory_space_constraint(w_gate, pltpu.VMEM)
    return pl.pallas_call(
        expert_body,
        grid=(n_rows // tile,),
        in_specs=[
            pl.BlockSpec((tile, width), lambda i: (i, 0)),
            pl.BlockSpec(memory_space=pltpu.VMEM),
            pl.BlockSpec((width, hidden), lambda i: (0, 0)),
            pl.BlockSpec((hidden, width), lambda i: (0, 0)),
        ],
        out_specs=pl.BlockSpec((tile, width), lambda i: (i, 0)),
        out_shape=jax.ShapeDtypeStruct((n_rows, width), BF16),
        compiler_params=pltpu.CompilerParams(vmem_limit_bytes=62500000),
        cost_estimate=pl.CostEstimate(
            flops=6 * n_rows * width * hidden, bytes_accessed=12 << 20, transcendentals=0
        ),
        name="expert",
    )(rows, w_gate, w_up, w_down)


def expert_apply(rows, w_gate, w_up, w_down, dtype, n_rows=None):
    n_rows, width = n_rows or rows.shape[0], rows.shape[1]
    hidden = w_gate.shape[1]
    tile = min(512, n_rows)
    return pl.pallas_call(
        expert_body,
        grid=(n_rows // tile,),
        in_specs=[
            pl.BlockSpec((tile, width), lambda i: (i, 0)),
            pl.BlockSpec((width, hidden), lambda i: (0, 0)),
            pl.BlockSpec((width, hidden), lambda i: (0, 0)),
            pl.BlockSpec((hidden, width), lambda i: (0, 0)),
        ],
        out_specs=pl.BlockSpec((tile, width), lambda i: (i, 0)),
        out_shape=jax.ShapeDtypeStruct((n_rows, width), dtype),
        cost_estimate=pl.CostEstimate(
            flops=6 * n_rows * width * hidden, bytes_accessed=14 << 20, transcendentals=0
        ),
        compiler_params=ALL_VMEM,
        name="expert",
    )(rows, w_gate, w_up, w_down)


def combine_body(weight_ref, rows_ref, shared_ref, out_ref, total):
    both = dot(weight_ref[...], rows_ref[...])
    n_tokens = out_ref.shape[0]
    part = both[:n_tokens] + both[n_tokens:]

    @pl.when(pl.program_id(0) == 0)
    def _():
        total[...] = part + shared_ref[...]

    @pl.when(pl.program_id(0) == 1)
    def _():
        out_ref[...] = (total[...] + part).astype(BF16)


def combine(weights, rows, shared):
    n_slots, width = rows.shape
    n_tokens = shared.shape[0]
    tile = n_slots // 2
    return pl.pallas_call(
        combine_body,
        grid=(2,),
        in_specs=[
            pl.BlockSpec((2 * n_tokens, tile), lambda i: (0, i)),
            pl.BlockSpec((tile, width), lambda i: (i, 0)),
            pl.BlockSpec((n_tokens, width), lambda i: (0, 0)),
        ],
        out_specs=pl.BlockSpec((n_tokens, width), lambda i: (0, 0)),
        out_shape=jax.ShapeDtypeStruct((n_tokens, width), BF16),
        scratch_shapes=[pltpu.VMEM((n_tokens, width), F32)],
        compiler_params=ALL_VMEM,
        cost_estimate=pl.CostEstimate(
            flops=4 * n_tokens * n_slots * width, bytes_accessed=6 << 20, transcendentals=0
        ),
        name="combine",
    )(weights, rows, shared)


def exchange(x, axes):
    return lax.all_to_all(x, axes, split_axis=0, concat_axis=0, tiled=True)


def local(
    query_rows,
    key_rows,
    value_rows,
    gate_rows,
    log_decay,
    out_proj,
    moe_input,
    norm_gain,
    routing,
    route_weight,
    expert_gate,
    expert_up,
    expert_down,
    shared_gate,
    shared_up,
    shared_down,
):
    n_rows = query_rows.shape[0]
    width = moe_input.shape[1]
    tp = lax.axis_size("tp")
    experts = lax.axis_size(EP) * tp

    n_tokens = moe_input.shape[0]
    places = lax.axis_size(EP)
    routes, route_weights = routing.T, route_weight.T
    message = norm(moe_input, norm_gain, routes)
    messages = all_shifts(message, "tp")

    keep, give = end_state(key_rows, value_rows, log_decay)
    got = shift(give, "ep_2", 1)
    pair = join_cores(keep, got)
    pairs = all_shifts(pair, "ep_1")
    before, plane = join_plane(pairs)
    planes = all_shifts(plane, "ep_0")
    mine, give = join_last(planes, before, keep, got)
    theirs = shift(give, "ep_2", 1)

    outgoing = dispatch(messages[:1], (0,), places)
    outgoing = dispatch(messages[1:], (1, 2, 3), places, outgoing)
    received = exchange(outgoing.reshape(places, tp * CAP, width), EP)

    own, other = gather_projection(out_proj)

    retained = mixer(query_rows, key_rows, value_rows, gate_rows, log_decay, mine, theirs)
    retained = retained.reshape(tp, n_rows // tp, -1)
    place = lax.axis_index("tp")
    heads = []
    for d in range(1, tp):
        block = lax.dynamic_index_in_dim(retained, (place + d) % tp, keepdims=False)
        heads.append(shift(block, "tp", d))

    shared = expert_apply(message, shared_gate, shared_up, shared_down, F32, n_tokens)
    weights = slot_weights(routes, route_weights, experts * CAP)

    served = expert_held(received.reshape(-1, width), expert_gate[0], expert_up[0], expert_down[0])
    returned = exchange(served.reshape(experts, CAP, width), EP_TP)

    mixer_out = project(retained, heads, out_proj, own, other)
    moe_out = combine(weights, returned.reshape(-1, width), shared)
    return (mixer_out, moe_out)


def solution(mesh):
    split = Mesh(mesh.devices.reshape(4, 4, 2, mesh.shape["tp"]), ("ep_0", "ep_1", "ep_2", "tp"))
    return jax.shard_map(
        local,
        mesh=split,
        in_specs=(
            P(EP, "tp"),
            P(EP, "tp"),
            P(EP, "tp"),
            P(EP, "tp"),
            P("tp", EP),
            P("tp", None),
            P(EP_TP, None),
            P(),
            P(EP_TP, None),
            P(EP_TP, None),
            P(EP_TP, None, None),
            P(EP_TP, None, None),
            P(EP_TP, None, None),
            P(),
            P(),
            P(),
        ),
        out_specs=(P(EP_TP, None), P(EP_TP, None)),
        check_vma=False,
    )
```
